128 devices in a mesh: ep: 32 (over z, y, core), tp: 4 (over x).
Axes of the slice: x: 4, y: 4, z: 4, core: 2. Of those that a mesh axis runs over, the one named last changes fastest.
Arguments:
- tokens: bfloat16 [1024, 2048], P('ep'), may hold values from -6 to 6
- kv_cache: bfloat16 [1024, 1024, 512], P('ep', None, 'tp'), may hold values from -320 to 320
- lengths: int32 [1024], P('ep'), may hold values from 1 to 1024, 524288 in all
- attn_gain: float32 [2048], replicated, may hold values from 0.1 to 1.9
- w_query: bfloat16 [2048, 1024], P(None, 'tp'), may hold values from -0.125 to 0.125
- w_key: bfloat16 [2048, 256], P(None, 'tp'), may hold values from -0.125 to 0.125
- w_value: bfloat16 [2048, 256], P(None, 'tp'), may hold values from -0.125 to 0.125
- lambdas: float32 [16], P('tp'), may hold values from 0.3 to 0.8
- head_gain: float32 [64], replicated, may hold values from 0.1 to 1.9
- w_out: bfloat16 [1024, 2048], replicated, may hold values from -0.1875 to 0.1875
- ffn_gain: float32 [2048], replicated, may hold values from 0.1 to 1.9
- w_shared_gate: bfloat16 [2048, 512], P(None, 'tp'), may hold values from -0.125 to 0.125
- w_shared_up: bfloat16 [2048, 512], P(None, 'tp'), may hold values from -0.125 to 0.125
- w_shared_down: bfloat16 [512, 2048], P('tp'), may hold values from -0.25 to 0.25
- routing: int32 [1024, 4], replicated, may hold values from 0 to 127, all different within a row; in each aligned block of 32 rows (0 to 31, 32 to 63, ...) at most 2 rows name the same one
- route_weights: float32 [1024, 4], P('ep'), may hold values from 0.1 to 1
- w_exp_gate: bfloat16 [128, 2048, 512], P(('ep', 'tp')), may hold values from -0.125 to 0.125
- w_exp_up: bfloat16 [128, 2048, 512], P(('ep', 'tp')), may hold values from -0.125 to 0.125
- w_exp_down: bfloat16 [128, 512, 2048], P(('ep', 'tp')), may hold values from -0.25 to 0.25
Outputs:
- mixed: bfloat16 [1024, 2048], P('ep', 'tp')
The draws below stay inside these ranges and needn't reach their ends.
Inputs may be any that keep to these rules, and one draw needn't show every extreme that they name: `lengths`: A sequence's cache holds its past keys and values at positions below its length, and the new token follows them; some sequence uses all 1024 positions. `routing`: each row names 4 different experts. Within the rows of one group of 32 sequences (aligned blocks) no expert is named by more than 2 rows, and in some blocks an expert is named by exactly 2.
All inputs are finite; a program needn't handle non-finite values. No bound on the sum of `lengths` on one device may be relied on, other than what follows from the above.
Results may differ from the reference program's by a relative error of at most 0.015.
The reference program's roundings to bfloat16 on the way count: a program that leaves them out, or rounds other values in their place, can miss the bound.
Values may be sent and summed in bfloat16 or wider, within the bound.
No kernel may reach another device: no remote copies, remote signals or barrier semaphores. Data moves between devices by JAX's collectives and lax.ppermute only.
A program may use at most 128 MiB of HBM per device.

```python
import math
import jax
import jax.numpy as jnp
import numpy as np
from jax import lax

D = 2048
HEADS = 16
KV_HEADS = 4
QK_DIM = 32
V_DIM = 64
FF_S = 512
FF_E = 512
TOPK = 4
SEQ_DEV = 32
CACHE = 1024
BATCH = 1024
EXPERTS = 128
CAP = 2
N_EP = 32
N_TP = 4


def draw_kv_cache(key, part):
    key_base = jax.random.fold_in(key, 0)
    full_shape = (BATCH, CACHE, KV_HEADS, 2, 2 * QK_DIM)
    base_draw = jax.random.normal(key_base, full_shape, jnp.float32)
    scales = jnp.array([1.75, 1.0], jnp.float32)
    entries = base_draw * scales[:, None]
    return entries.reshape(BATCH, CACHE, KV_HEADS * 4 * QK_DIM).astype(jnp.bfloat16)


def steps_of(key, dims, cuts, smallest, top_value):
    loudness = 1.0
    for dim, blocks in cuts:
        draws = jax.random.uniform(jax.random.fold_in(jax.random.fold_in(key, 6), dim), (blocks,), jnp.float32, smallest / len(cuts), top_value / len(cuts))
        loudness = loudness * jnp.repeat(jnp.exp(draws), dims[dim] // blocks).reshape((-1,) + (1,) * (len(dims) - 1 - dim))
    return loudness


def split_up(amount, total, reach, slope):
    loads = [(1 << 20) // math.isqrt(grade ** slope) + 1 for grade in range(2, amount + 1)]
    spare, counts = total - reach - (amount - 1), [1] * (amount - 1)
    while spare > 0:
        free = [i for i in range(amount - 1) if counts[i] < reach]
        mass, left = sum([loads[i] for i in free]), spare
        for i in free:
            extra = min(reach - counts[i], max(1, left * loads[i] // mass), spare)
            counts[i] = counts[i] + extra
            spare = spare - extra
    return np.array([reach] + counts)


def ragged_sizes(stream_key, number_of, total, most, lean):
    if number_of == 2:
        one = jax.random.randint(stream_key, (), max(1, total - most), min(most, total - 1) + 1)
        return jnp.stack([one, total - one])
    sizes = jnp.asarray(split_up(number_of, total, most, lean), jnp.int32)
    couples = (number_of - 1) // 2
    giver, taker = sizes[1:1 + 2 * couples:2], sizes[2:2 + 2 * couples:2]
    slack = jnp.minimum(giver - 1, most - taker)
    moved = jax.random.randint(jax.random.fold_in(stream_key, 1), (couples,), 0, 1 << 20) % (slack + 1)
    sizes = sizes.at[1:1 + 2 * couples:2].set(giver - moved).at[2:2 + 2 * couples:2].set(taker + moved)
    return sizes[jax.random.permutation(jax.random.fold_in(stream_key, 2), number_of)]


def shared_out(own_key, own, number, rows, number_of, top, bound, skew):
    sequence = jax.random.permutation(own_key, number_of)
    packed, common = load_shares(number_of, rows * top, bound, skew, True), load_shares(number_of, rows * top, bound, skew, False)
    places = jnp.arange(number_of)

    def named(sizes, rotation):
        used = int((sizes > 0).sum())
        fixed = max(1, used // 4)
        shifted = fixed + (places - fixed + rotation * (used - fixed)) % max(1, number_of - fixed)
        return jnp.zeros((number_of,), jnp.int32).at[sequence[jnp.where(places < fixed, places, shifted)]].set(jnp.asarray(sizes, jnp.int32))

    sizes = jnp.where(number % 4 == 0, named(packed, number // 4), named(common, number - number // 4 - 1))
    mixed = jax.random.permutation(jax.random.fold_in(own, 3), number_of)
    source_of, taker = mixed[0:number_of // 2 * 2:2], mixed[1:number_of // 2 * 2:2]
    room = jnp.minimum(sizes[source_of] - 1, bound - sizes[taker]) // 2
    room = jnp.where((source_of == sequence[0]) | (taker == sequence[0]) | (sizes[taker] == 0), 0, jnp.maximum(room, 0))
    shifted = jax.random.randint(jax.random.fold_in(own, 4), (number_of // 2,), 0, 1 << 20) % (room + 1)
    sizes = sizes.at[source_of].add(-shifted).at[taker].add(shifted)
    labels = jnp.searchsorted(jnp.cumsum(sizes), jnp.arange(rows * top), side="right").astype(jnp.int32)
    table = labels.reshape(top, rows).T
    table = table[jax.random.permutation(jax.random.fold_in(own, 1), rows)]
    rotation = jax.random.randint(jax.random.fold_in(own, 2), (rows, 1), 0, top)
    return jnp.take_along_axis(table, (jnp.arange(top)[None, :] + rotation) % top, axis=1)


def load_shares(count, total, reach, lean, full):
    loads = [(1 << 20) // math.isqrt(rank ** lean) + 1 for rank in range(1, count + 1)]
    largest = reach if full else min(reach, max(-(-total // count), total * loads[0] // sum(loads)))
    least = 1 if total - largest >= count - 1 else 0
    holding, rest = [largest] + [least] * (count - 1), total - largest - least * (count - 1)
    while rest > 0:
        movable = [i for i in range(1, count) if holding[i] < largest] or [i for i in range(1, count) if holding[i] < reach]
        whole, left = sum([loads[i] for i in movable]), rest
        for i in movable:
            extra = min(reach - holding[i], max(1, left * loads[i] // whole), rest)
            holding[i] = holding[i] + extra
            rest = rest - extra
    return np.array(holding)


def normal_values(stream_key, extent, width, bound, cuts=(), kind=jnp.bfloat16):
    drawn = width * jax.random.normal(stream_key, extent, jnp.float32)
    if cuts:
        drawn = drawn * steps_of(stream_key, extent, cuts, -0.22, 0.18)
    return jnp.clip(drawn, -bound, bound).astype(kind)


def setup_inputs(seed: int = 0) -> dict:
    streams_of = jax.random.split(jax.random.key(seed), 20)
    tokens = normal_values(streams_of[0], (BATCH, D), 1.0, 6.0, ((0, 32),))
    kv_cache = draw_kv_cache(jax.random.fold_in(streams_of[19], 71), 0)
    lengths = ragged_sizes(streams_of[2], BATCH, BATCH * CACHE // 2, CACHE, 2).astype(jnp.int32)
    attn_gain = jnp.clip(1.0 + 0.18 * jax.random.normal(streams_of[3], (D,), jnp.float32), 0.1, 1.9)
    w_query = normal_values(streams_of[4], (D, HEADS * 2 * QK_DIM), D ** -0.5, 0.125, ((1, 4),))
    w_key = normal_values(streams_of[5], (D, KV_HEADS * 2 * QK_DIM), D ** -0.5, 0.125, ((1, 4),))
    w_value = normal_values(streams_of[6], (D, KV_HEADS * V_DIM), D ** -0.5, 0.125, ((1, 4),))
    lambdas = jnp.clip(0.3 + 0.5 * jax.random.uniform(streams_of[7], (HEADS,), jnp.float32) ** steps_of(streams_of[7], (HEADS,), ((0, 4),), -0.2, 0.2), 0.3, 0.8)
    head_gain = jnp.clip(1.0 + 0.18 * jax.random.normal(streams_of[8], (V_DIM,), jnp.float32), 0.1, 1.9)
    w_out = normal_values(streams_of[9], (HEADS * V_DIM, D), (HEADS * V_DIM) ** -0.5, 0.1875)
    ffn_gain = jnp.clip(1.0 + 0.18 * jax.random.normal(streams_of[10], (D,), jnp.float32), 0.1, 1.9)
    w_shared_gate = normal_values(streams_of[11], (D, FF_S), D ** -0.5, 0.125, ((1, 4),))
    w_shared_up = normal_values(streams_of[12], (D, FF_S), D ** -0.5, 0.125, ((1, 4),))
    w_shared_down = normal_values(streams_of[13], (FF_S, D), FF_S ** -0.5, 0.25, ((0, 4),))
    routing_keys = jax.random.split(jax.random.fold_in(streams_of[14], 1), BATCH // SEQ_DEV)
    routing_turns = jax.random.permutation(jax.random.fold_in(streams_of[14], 3), BATCH // SEQ_DEV)
    routing = jax.vmap(lambda own, number: shared_out(jax.random.fold_in(streams_of[14], 2), own, number, SEQ_DEV, EXPERTS, TOPK, CAP, 2))(routing_keys, routing_turns).reshape((BATCH, TOPK))
    route_weights = jnp.clip(jnp.exp(math.log(1.0) - 2.3025851 * jax.random.uniform(streams_of[15], (BATCH, TOPK), jnp.float32) ** steps_of(streams_of[15], (BATCH, TOPK), ((0, 32),), -0.2, 0.2)), 0.1, 1.0)
    w_exp_gate = normal_values(streams_of[16], (EXPERTS, D, FF_E), D ** -0.5, 0.125, ((0, 128),))
    w_exp_up = normal_values(streams_of[17], (EXPERTS, D, FF_E), D ** -0.5, 0.125, ((0, 128),))
    w_exp_down = normal_values(streams_of[18], (EXPERTS, FF_E, D), FF_E ** -0.5, 0.25, ((0, 128),))
    return {"tokens": tokens, "kv_cache": kv_cache, "lengths": lengths, "attn_gain": attn_gain, "w_query": w_query, "w_key": w_key, "w_value": w_value, "lambdas": lambdas, "head_gain": head_gain, "w_out": w_out, "ffn_gain": ffn_gain, "w_shared_gate": w_shared_gate, "w_shared_up": w_shared_up, "w_shared_down": w_shared_down, "routing": routing, "route_weights": route_weights, "w_exp_gate": w_exp_gate, "w_exp_up": w_exp_up, "w_exp_down": w_exp_down}


epsilon = 1e-06
neg_fill = -1e+30

def norm_rows(values, gain_vec):
    widened = values.astype(jnp.float32)
    return widened * lax.rsqrt(lax.optimization_barrier(jnp.mean(widened * widened, axis=-1, keepdims=True)) + epsilon) * gain_vec

def group_sum(inner_act, weight):
    row_count = inner_act.shape[0]
    pieces = jnp.einsum('mtf,tfd->mtd', inner_act.reshape(row_count, N_TP, -1).astype(jnp.float32), weight.reshape(N_TP, -1, weight.shape[-1]).astype(jnp.float32))
    rounded = lax.optimization_barrier(pieces.astype(jnp.bfloat16))
    return lax.optimization_barrier(jnp.sum(rounded.astype(jnp.float32), axis=1))

def attend(block_q, block_k, block_v, block_cache, block_len, lambdas, head_gain):
    seq_total = block_q.shape[0]
    v_width = head_gain.shape[0]
    qk_width = v_width // 2
    kv_total = block_cache.shape[2] // (2 * v_width)
    group_size = lambdas.shape[0] // kv_total
    cache_len = block_cache.shape[1]
    queries = block_q.reshape(seq_total, kv_total, group_size, 2, qk_width).astype(jnp.float32)
    key_new = block_k.reshape(seq_total, kv_total, 2, qk_width).astype(jnp.float32)
    value_new = block_v.reshape(seq_total, kv_total, v_width).astype(jnp.float32)
    layout = block_cache.reshape(seq_total, cache_len, kv_total, 2 * v_width)
    keys_old = layout[..., :v_width].reshape(seq_total, cache_len, kv_total, 2, qk_width).astype(jnp.float32)
    values_old = layout[..., v_width:].astype(jnp.float32)
    scaling = qk_width ** (-0.5)
    scores_old = jnp.einsum('skgmd,sckmd->skgmc', queries, keys_old) * scaling
    scores_new = jnp.einsum('skgmd,skmd->skgm', queries, key_new) * scaling
    position = jnp.arange(cache_len, dtype=jnp.int32)
    valid_mask = (position[None, :] < block_len[:, None])[:, None, None, None, :]
    scores_old = jnp.where(valid_mask, scores_old, neg_fill)
    highest = jnp.maximum(lax.optimization_barrier(jnp.max(scores_old, axis=-1)), scores_new)
    expo_old = jnp.where(valid_mask, jnp.exp(scores_old - highest[..., None]), 0.0)
    expo_new = jnp.exp(scores_new - highest)
    totals = lax.optimization_barrier(jnp.sum(expo_old, axis=-1)) + expo_new
    lambda_grid = lambdas.reshape(kv_total, group_size)[None, :, :]
    weight_old = (expo_old[..., 0, :] / totals[..., 0, None] - lambda_grid[..., None] * expo_old[..., 1, :] / totals[..., 1, None]).astype(jnp.bfloat16)
    weight_new = (expo_new[..., 0] / totals[..., 0] - lambda_grid * expo_new[..., 1] / totals[..., 1]).astype(jnp.bfloat16)
    head_mix = jnp.einsum('skgc,sckv->skgv', weight_old.astype(jnp.float32), values_old)
    head_mix = head_mix + weight_new.astype(jnp.float32)[..., None] * value_new[:, :, None, :]
    return norm_rows(head_mix, head_gain).astype(jnp.bfloat16).reshape(seq_total, -1)

def reference(tokens, kv_cache, lengths, attn_gain, w_query, w_key, w_value, lambdas, head_gain, w_out, ffn_gain, w_shared_gate, w_shared_up, w_shared_down, routing, route_weights, w_exp_gate, w_exp_up, w_exp_down):
    normed = norm_rows(tokens, attn_gain).astype(jnp.bfloat16)
    queries = jnp.dot(normed, w_query, preferred_element_type=jnp.float32).astype(jnp.bfloat16)
    key_new = jnp.dot(normed, w_key, preferred_element_type=jnp.float32).astype(jnp.bfloat16)
    value_new = jnp.dot(normed, w_value, preferred_element_type=jnp.float32).astype(jnp.bfloat16)

    def attend_block(operands):
        return attend(operands[0], operands[1], operands[2], operands[3], operands[4], lambdas, head_gain)
    head_out = lax.map(attend_block, (queries.reshape(N_EP, SEQ_DEV, -1), key_new.reshape(N_EP, SEQ_DEV, -1), value_new.reshape(N_EP, SEQ_DEV, -1), kv_cache.reshape(N_EP, SEQ_DEV, CACHE, -1), lengths.reshape(N_EP, SEQ_DEV)))
    head_out = head_out.reshape(BATCH, HEADS * V_DIM)
    projected = group_sum(head_out, w_out)
    residual = (tokens.astype(jnp.float32) + projected).astype(jnp.bfloat16)
    ffn_in = norm_rows(residual, ffn_gain).astype(jnp.bfloat16)
    gate_vals = jnp.dot(ffn_in, w_shared_gate, preferred_element_type=jnp.float32)
    up_vals = jnp.dot(ffn_in, w_shared_up, preferred_element_type=jnp.float32)
    shared_act = (jax.nn.silu(gate_vals) * up_vals).astype(jnp.bfloat16)
    shared = jnp.dot(shared_act, w_shared_down, preferred_element_type=jnp.float32)
    grouped_ids = routing.reshape(N_EP, SEQ_DEV * TOPK)
    onehot = (grouped_ids[..., None] == jnp.arange(EXPERTS, dtype=jnp.int32)).astype(jnp.int32)
    slot_rank = lax.optimization_barrier(jnp.sum((jnp.cumsum(onehot, axis=1) - onehot) * onehot, axis=-1)).astype(jnp.int32)
    group_ids = jnp.broadcast_to(jnp.arange(N_EP, dtype=jnp.int32)[:, None], slot_rank.shape)
    rows_in = jnp.repeat(ffn_in.reshape(N_EP, SEQ_DEV, D), TOPK, axis=1)
    buffers = jnp.zeros((EXPERTS, N_EP, CAP, D), jnp.bfloat16).at[grouped_ids, group_ids, slot_rank].set(rows_in)

    def expert_apply(operands):
        row_block, gate_w, up_w, down_w = operands
        flat_rows = row_block.reshape(N_EP * CAP, D)
        gate_part = jnp.dot(flat_rows, gate_w, preferred_element_type=jnp.float32)
        up_part = jnp.dot(flat_rows, up_w, preferred_element_type=jnp.float32)
        inner_act = (jax.nn.silu(gate_part) * up_part).astype(jnp.bfloat16)
        result = jnp.dot(inner_act, down_w, preferred_element_type=jnp.float32).astype(jnp.bfloat16)
        return result.reshape(N_EP, CAP, D)
    expert_res = lax.map(expert_apply, (buffers, w_exp_gate, w_exp_up, w_exp_down))
    picked = expert_res[grouped_ids, group_ids, slot_rank].astype(jnp.float32)
    routed = lax.optimization_barrier(jnp.sum(route_weights.reshape(N_EP, SEQ_DEV, TOPK, 1) * picked.reshape(N_EP, SEQ_DEV, TOPK, D), axis=2))
    routed = routed.reshape(BATCH, D)
    return (residual.astype(jnp.float32) + shared + routed).astype(jnp.bfloat16)
```

```python
import jax
import jax.numpy as jnp
from jax import lax
from jax.sharding import PartitionSpec as P

epsilon = 1e-06
neg_fill = -1e30


def in_order(tiles, dim):
    tiles = jnp.moveaxis(tiles, 0, dim)
    lengths = tiles.shape
    return tiles.reshape(*lengths[:dim], lengths[dim] * lengths[dim + 1], *lengths[dim + 2 :])


def sent_to_all(shard, axis):
    copies = jnp.broadcast_to(shard, (lax.axis_size(axis), *shard.shape))
    return lax.all_to_all(copies, axis, split_axis=0, concat_axis=0, tiled=True)


def gathered_copies(shard, axis, dim):
    return in_order(sent_to_all(shard, axis), dim)


def cut_along(shard, dim, count):
    lengths = shard.shape
    tiles = shard.reshape(*lengths[:dim], count, lengths[dim] // count, *lengths[dim + 1 :])
    return jnp.moveaxis(tiles, dim, 0)


def sent_and_summed(shard, axis, dim):
    count = lax.axis_size(axis)
    tiles = lax.all_to_all(cut_along(shard, dim, count), axis, 0, 0, tiled=True)
    return jnp.sum(tiles.astype(jnp.float32), axis=0)


def norm_rows(values, gain_vec):
    widened = values.astype(jnp.float32)
    return (
        widened
        * lax.rsqrt(jnp.mean(widened * widened, axis=-1, keepdims=True) + epsilon)
        * gain_vec
    )


def attention(normed, kv_cache, lengths, w_query, w_key, w_value, lambdas, head_gain):
    seq_count = normed.shape[0]
    v_width = head_gain.shape[0]
    qk_width = v_width // 2
    kv_local = kv_cache.shape[2] // (2 * v_width)
    head_local = lambdas.shape[0]
    group_size = head_local // kv_local
    cache_len = kv_cache.shape[1]
    queries = jnp.dot(normed, w_query, preferred_element_type=jnp.float32).astype(jnp.bfloat16)
    queries = queries.reshape(seq_count, kv_local, group_size, 2, qk_width)
    key_new = jnp.dot(normed, w_key, preferred_element_type=jnp.float32).astype(jnp.bfloat16)
    key_new = key_new.reshape(seq_count, kv_local, 2, qk_width)
    value_new = jnp.dot(normed, w_value, preferred_element_type=jnp.float32).astype(jnp.bfloat16)
    value_new = value_new.reshape(seq_count, kv_local, v_width)
    layout = kv_cache.reshape(seq_count, cache_len, kv_local, 2 * v_width)
    keys_old = layout[..., :v_width].reshape(seq_count, cache_len, kv_local, 2, qk_width)
    values_old = layout[..., v_width:]
    scaling = qk_width ** (-0.5)
    scores_old = (
        jnp.einsum("skgmd,sckmd->skgmc", queries, keys_old, preferred_element_type=jnp.float32)
        * scaling
    )
    scores_new = (
        jnp.einsum("skgmd,skmd->skgm", queries, key_new, preferred_element_type=jnp.float32)
        * scaling
    )
    position = jnp.arange(cache_len, dtype=jnp.int32)
    valid_mask = (position[None, :] < lengths[:, None])[:, None, None, None, :]
    scores_old = jnp.where(valid_mask, scores_old, neg_fill)
    highest = jnp.maximum(jnp.max(scores_old, axis=-1), scores_new)
    expo_old = jnp.where(valid_mask, jnp.exp(scores_old - highest[..., None]), 0.0)
    expo_new = jnp.exp(scores_new - highest)
    totals = jnp.sum(expo_old, axis=-1) + expo_new
    lambda_grid = lambdas.reshape(kv_local, group_size)[None, :, :]
    weight_old = (
        expo_old[..., 0, :] / totals[..., 0, None]
        - lambda_grid[..., None] * expo_old[..., 1, :] / totals[..., 1, None]
    ).astype(jnp.bfloat16)
    weight_new = (
        expo_new[..., 0] / totals[..., 0] - lambda_grid * expo_new[..., 1] / totals[..., 1]
    ).astype(jnp.bfloat16)
    head_mix = jnp.einsum(
        "skgc,sckv->skgv", weight_old, values_old, preferred_element_type=jnp.float32
    )
    head_mix = (
        head_mix
        + weight_new.astype(jnp.float32)[..., None] * value_new.astype(jnp.float32)[:, :, None, :]
    )
    return (
        norm_rows(head_mix, head_gain).astype(jnp.bfloat16).reshape(seq_count, head_local * v_width)
    )


def shards(
    tokens,
    kv_cache,
    lengths,
    attn_gain,
    w_query,
    w_key,
    w_value,
    lambdas,
    head_gain,
    w_out,
    ffn_gain,
    w_shared_gate,
    w_shared_up,
    w_shared_down,
    routing,
    route_weights,
    w_exp_gate,
    w_exp_up,
    w_exp_down,
):
    seq_count = tokens.shape[0]
    width = tokens.shape[1]
    tp_count = lax.axis_size("tp")
    tp_index = lax.axis_index("tp")
    ep_count = lax.axis_size("ep")
    ep_index = lax.axis_index("ep")
    experts = ep_count * tp_count
    capacity = 2
    width_share = width // tp_count
    normed = norm_rows(tokens, attn_gain).astype(jnp.bfloat16)
    head_out = attention(normed, kv_cache, lengths, w_query, w_key, w_value, lambdas, head_gain)
    share_rows = head_out.shape[1]
    own_routing = lax.dynamic_slice_in_dim(routing, ep_index * seq_count, seq_count, 0)
    hits = own_routing[:, :, None] == jnp.arange(experts, dtype=jnp.int32)[None, None, :]
    named = jnp.any(hits, axis=1).astype(jnp.bfloat16)
    earlier = (
        jnp.arange(seq_count)[:, None] > jnp.arange(seq_count)[None, :]
    ).astype(jnp.bfloat16)
    rank = jnp.dot(earlier, named, preferred_element_type=jnp.float32)
    rank_ok = rank[:, :, None] == jnp.arange(capacity, dtype=jnp.float32)[None, None, :]
    placed = (named[:, :, None] > 0) & rank_ok
    dispatch = placed.astype(jnp.bfloat16).reshape(seq_count, experts * capacity)
    selector = (hits[:, :, :, None] & rank_ok[:, None, :, :]).astype(jnp.bfloat16)
    selector = selector.reshape(seq_count * hits.shape[1], experts * capacity)
    own_tokens = lax.dynamic_slice_in_dim(tokens, tp_index * width_share, width_share, 1)
    rows = jnp.concatenate([head_out, own_tokens], axis=1)
    packed = jnp.einsum("sj,sd->jd", dispatch, rows, preferred_element_type=jnp.float32).astype(
        jnp.bfloat16
    )
    packed = packed.reshape(experts, capacity, share_rows + width_share)
    arrived = lax.all_to_all(packed, ("ep", "tp"), split_axis=0, concat_axis=0, tiled=True)

    def project(parts):
        pieces = jnp.einsum(
            "tmk,tkd->tmd",
            parts,
            w_out.reshape(tp_count, share_rows, -1),
            preferred_element_type=jnp.float32,
        )
        rounded = lax.optimization_barrier(pieces.astype(jnp.bfloat16))
        return jnp.sum(rounded.astype(jnp.float32), axis=0)

    all_heads = sent_to_all(head_out, "tp")
    residual = (tokens.astype(jnp.float32) + project(all_heads)).astype(jnp.bfloat16)
    ffn_in = norm_rows(residual, ffn_gain).astype(jnp.bfloat16)
    gate_vals = jnp.dot(ffn_in, w_shared_gate, preferred_element_type=jnp.float32)
    up_vals = jnp.dot(ffn_in, w_shared_up, preferred_element_type=jnp.float32)
    shared_act = (jax.nn.silu(gate_vals) * up_vals).astype(jnp.bfloat16)
    shared_part = jnp.dot(shared_act, w_shared_down, preferred_element_type=jnp.float32)
    shared = sent_and_summed(shared_part.astype(jnp.bfloat16), "tp", 1)
    own_resid = lax.dynamic_slice_in_dim(residual, tp_index * width_share, width_share, 1)
    base = own_resid.astype(jnp.float32) + shared

    slots = ep_count * capacity
    parts = arrived.reshape(ep_count, tp_count, capacity, -1).transpose(1, 0, 2, 3)
    parts = parts.reshape(tp_count, slots, -1)
    row_tokens = in_order(parts[:, :, share_rows:], 1)
    row_resid = (row_tokens.astype(jnp.float32) + project(parts[:, :, :share_rows])).astype(
        jnp.bfloat16
    )
    flat_rows = norm_rows(row_resid, ffn_gain).astype(jnp.bfloat16)
    gate_part = jnp.dot(flat_rows, w_exp_gate[0], preferred_element_type=jnp.float32)
    up_part = jnp.dot(flat_rows, w_exp_up[0], preferred_element_type=jnp.float32)
    inner_act = (jax.nn.silu(gate_part) * up_part).astype(jnp.bfloat16)
    result = jnp.dot(inner_act, w_exp_down[0], preferred_element_type=jnp.float32).astype(
        jnp.bfloat16
    )
    computed = result.reshape(ep_count, capacity, tp_count, width_share).transpose(0, 2, 1, 3)
    computed = computed.reshape(experts, capacity, width_share)
    returned = lax.all_to_all(computed, ("ep", "tp"), split_axis=0, concat_axis=0, tiled=True)
    routed_rows = jnp.dot(
        selector,
        returned.reshape(experts * capacity, width_share),
        preferred_element_type=jnp.float32,
    ).reshape(seq_count, -1, width_share)
    routed = jnp.sum(route_weights[:, :, None] * routed_rows, axis=1)
    return (base + routed).astype(jnp.bfloat16)


def solution(mesh):
    return jax.shard_map(
        shards,
        mesh=mesh,
        in_specs=(
            P("ep", None),
            P("ep", None, "tp"),
            P("ep"),
            P(),
            P(None, "tp"),
            P(None, "tp"),
            P(None, "tp"),
            P("tp"),
            P(),
            P(),
            P(),
            P(None, "tp"),
            P(None, "tp"),
            P("tp", None),
            P(),
            P("ep", None),
            P(("ep", "tp"), None, None),
            P(("ep", "tp"), None, None),
            P(("ep", "tp"), None, None),
        ),
        out_specs=P("ep", "tp"),
        check_vma=False,
    )
```

```python
import jax
import jax.numpy as jnp
from jax import lax
from jax.experimental import pallas as pl
from jax.experimental.pallas import tpu as pltpu
from jax.sharding import PartitionSpec as P

epsilon = 1e-06
neg_fill = -1e30
SPAN = 512


def attend_kernel(
    lengths_hbm,
    lambdas_hbm,
    tokens_hbm,
    gain_hbm,
    w_query_hbm,
    w_key_hbm,
    w_value_hbm,
    head_gain_hbm,
    routing_hbm,
    route_weights_hbm,
    kv_hbm,
    message,
    heads,
    combine,
    kv,
    lengths,
    lambdas,
    tokens,
    gain,
    w_query,
    w_key,
    w_value,
    head_gain,
    routing,
    route_weights,
    q8,
    n4,
    spread,
    scores,
    turned,
    mix,
    sems,
    kv_sems,
):
    seqs, _ = tokens.shape
    cache_len = kv.shape[1]
    place = (lax.axis_index("ep"), lax.axis_index("tp"))
    spans = cache_len // SPAN
    rows_all = seqs * 4

    def kv_copy(i):
        part = pl.ds(i * SPAN, SPAN)
        return pltpu.make_async_copy(kv_hbm.at[:, part], kv.at[:, part], kv_sems.at[i])

    base = pl.multiple_of((place[0] // 4) * 128, 128)
    loads = [
        pltpu.make_async_copy(src, dst, sems.at[i])
        for i, (src, dst) in enumerate(
            [
                (tokens_hbm, tokens),
                (gain_hbm, gain),
                (w_query_hbm, w_query),
                (w_key_hbm, w_key),
                (w_value_hbm, w_value),
                (head_gain_hbm, head_gain),
                (routing_hbm.at[:, pl.ds(base, 128)], routing),
                (route_weights_hbm, route_weights),
                (lengths_hbm, lengths),
                (lambdas_hbm, lambdas),
            ]
        )
    ]
    for load in loads:
        load.start()
    for i in range(spans):
        kv_copy(i).start()

    lane = lax.broadcasted_iota(jnp.int32, (1, 128), 1)
    loads[0].wait()
    loads[1].wait()
    wide = tokens[...].astype(jnp.float32)
    scale = lax.rsqrt(jnp.mean(wide * wide, axis=1, keepdims=True) + epsilon)
    normed = (wide * scale * gain[...]).astype(jnp.bfloat16)
    for load in loads[2:]:
        load.wait()

    def rounded(value):
        return value.astype(jnp.bfloat16).astype(jnp.float32)

    def against(weight):
        return rounded(
            lax.dot_general(
                normed,
                weight[...],
                (((1,), (1,)), ((), ())),
                preferred_element_type=jnp.float32,
            )
        )

    queries = rounded(jnp.dot(normed, w_query[...], preferred_element_type=jnp.float32))
    new_row = jnp.concatenate([against(w_key), against(w_value)], axis=1)
    for head in range(4):
        pair = queries[:, 128 * (head // 2) : 128 * (head // 2) + 128]
        if head % 2:
            pair = pltpu.roll(pair, 64, 1)
        for half in range(2):
            own = (lane >= 32 * half) & (lane < 32 * half + 32)
            q8[pl.ds(half * rows_all + head, seqs, stride=4), :] = jnp.where(own, pair, 0.0)
        n4[pl.ds(head, seqs, stride=4), :] = new_row
    query_t = [q8[half * rows_all : (half + 1) * rows_all, :].T for half in range(2)]
    fresh = n4[...]
    fresh_t = fresh.T
    lane_seq = lax.broadcasted_iota(jnp.int32, (64, 128), 1) // 4
    for half in range(2):
        for s in range(seqs):
            spread[s * 64 : (s + 1) * 64, half * 128 : half * 128 + 128] = jnp.where(
                lane_seq == s, query_t[half][:64], 0.0
            ).astype(jnp.bfloat16)

    shift = 128 - (place[0] % 4) * 32
    named = jnp.where(lane < seqs, pltpu.roll(routing[...], shift, 1), -1)
    slot_row = lax.broadcasted_iota(jnp.int32, (256, 128), 0)
    slot_expert = slot_row // 2
    any_at = slot_expert == named[0:1, :]
    for k in range(1, 4):
        any_at = any_at | (slot_expert == named[k : k + 1, :])
    at_row = lax.broadcasted_iota(jnp.int32, (128, 128), 0)
    at_column = lax.broadcasted_iota(jnp.int32, (128, 128), 1)
    before = (at_row < at_column).astype(jnp.float32).astype(jnp.bfloat16)
    rank = jnp.dot(
        any_at.astype(jnp.float32).astype(jnp.bfloat16),
        before,
        preferred_element_type=jnp.float32,
    )
    parity = (slot_row % 2).astype(jnp.float32)
    taken = any_at & (rank == parity)
    picks = jnp.where(taken, 1.0, 0.0).astype(jnp.bfloat16)[:, :seqs]
    amount = jnp.zeros((256, 128), jnp.float32)
    widths = jnp.concatenate([route_weights[...]] * 4, axis=1)
    for k in range(4):
        amount = jnp.where(slot_expert == named[k : k + 1, :], widths[k : k + 1, :], amount)
    amount = jnp.where(taken, amount, 0.0).T[:seqs, :]
    for k in range(3):
        term = amount.astype(jnp.bfloat16)
        combine[k * seqs : (k + 1) * seqs, :] = term
        amount = amount - term.astype(jnp.float32)

    scaling = 32 ** (-0.5)
    count = jnp.zeros((1, 128), jnp.int32)
    for s in range(seqs):
        count = jnp.where(lane // 4 == s, lengths[s], count)
    count = jnp.concatenate([count, count], axis=1)
    lam = jnp.zeros((1, 128), jnp.float32)
    for head in range(4):
        lam = jnp.where(lane % 4 == head, lambdas[head], lam)
    score_new = [
        jnp.sum(query_t[half] * fresh_t, axis=0, keepdims=True) * scaling for half in range(2)
    ]
    score_new = jnp.concatenate(score_new, axis=1)

    position = lax.broadcasted_iota(jnp.int32, (SPAN, 256), 0)
    highest = score_new
    for i in range(spans):
        kv_copy(i).wait()
        cut = slice(i * SPAN, (i + 1) * SPAN)
        part = jnp.concatenate([kv[s, cut, :64] for s in range(seqs)], axis=1)
        found = jnp.dot(part, spread[...], preferred_element_type=jnp.float32) * scaling
        found = jnp.where(position < count - i * SPAN, found, neg_fill)
        scores[i * SPAN : (i + 1) * SPAN, :] = found
        highest = jnp.maximum(highest, jnp.max(found, axis=0, keepdims=True))
    expo_new = jnp.exp(score_new - highest)
    total = expo_new
    for i in range(spans):
        found = scores[i * SPAN : (i + 1) * SPAN, :]
        expo = jnp.where(position < count - i * SPAN, jnp.exp(found - highest), 0.0)
        scores[i * SPAN : (i + 1) * SPAN, :] = expo
        total = total + jnp.sum(expo, axis=0, keepdims=True)
    factor = 1.0 / total
    first = factor[:, :128]
    second = lam * factor[:, 128:]
    for i in range(cache_len // 128):
        expo = scores[i * 128 : (i + 1) * 128, :]
        weight = expo[:, :128] * first - expo[:, 128:] * second
        turned[:, i * 128 : (i + 1) * 128] = weight.T.astype(jnp.bfloat16)
    weight_new = expo_new[:, :128] * first - expo_new[:, 128:] * second
    diagonal = jnp.where(at_row == at_column, weight_new, 0.0).astype(jnp.bfloat16)
    mix_new = jnp.dot(diagonal, fresh.astype(jnp.bfloat16), preferred_element_type=jnp.float32)
    upper = lax.broadcasted_iota(jnp.int32, (8, 1), 0) < 4
    for i in range(seqs // 2):
        both = jnp.concatenate([kv[2 * i], kv[2 * i + 1]], axis=1)
        out = jnp.dot(turned[8 * i : 8 * i + 8, :], both, preferred_element_type=jnp.float32)
        mix[8 * i : 8 * i + 8, :] = jnp.where(upper, out[:, :128], out[:, 128:])

    blend = mix[...] + mix_new
    values = jnp.where(lane >= 64, blend, 0.0)
    power = jnp.sum(values * values, axis=1, keepdims=True) * (1.0 / 64)
    gain2 = jnp.concatenate([head_gain[...], head_gain[...]], axis=1)
    mix[...] = blend * lax.rsqrt(power + epsilon) * gain2
    pieces = []
    for pair in range(2):
        even = mix[pl.ds(2 * pair, seqs, stride=4), :]
        odd = mix[pl.ds(2 * pair + 1, seqs, stride=4), :]
        both = jnp.where(lane < 64, pltpu.roll(even, 64, 1), odd).astype(jnp.bfloat16)
        heads[:, 128 * pair : 128 * pair + 128] = both
        pieces.append(both)
    first = pl.multiple_of(place[1] * 512, 128)
    share = tokens[:, pl.ds(first, 512)]
    source = jnp.concatenate(pieces + [share], axis=1)
    packed = jnp.dot(picks, source, preferred_element_type=jnp.float32).astype(jnp.bfloat16)
    for b in range(6):
        message[b] = packed[:, 128 * b : 128 * b + 128]


def in_hbm(*arrays):
    return [pltpu.with_memory_space_constraint(array, pltpu.HBM) for array in arrays]


def attend(
    tokens, kv_cache, lengths, gain, w_query, w_key, w_value, lambdas, head_gain, routing,
    route_weights,
):
    seqs, width = tokens.shape
    vmem = pl.BlockSpec(memory_space=pltpu.VMEM)
    hbm = pl.BlockSpec(memory_space=pltpu.HBM)
    bf16, f32 = jnp.bfloat16, jnp.float32
    return pl.pallas_call(
        attend_kernel,
        out_shape=(
            jax.ShapeDtypeStruct((6, 256, 128), bf16),
            jax.ShapeDtypeStruct((seqs, 256), bf16),
            jax.ShapeDtypeStruct((3 * seqs, 256), bf16),
        ),
        in_specs=[hbm] * 11,
        out_specs=(vmem, vmem, vmem),
        scratch_shapes=[
            pltpu.VMEM(kv_cache.shape, bf16),
            pltpu.SMEM((seqs,), jnp.int32),
            pltpu.SMEM((4,), f32),
            pltpu.VMEM((seqs, width), bf16),
            pltpu.VMEM((1, width), f32),
            pltpu.VMEM((width, 256), bf16),
            pltpu.VMEM((64, width), bf16),
            pltpu.VMEM((64, width), bf16),
            pltpu.VMEM((1, 64), f32),
            pltpu.VMEM((4, 128), jnp.int32),
            pltpu.VMEM((4, seqs), f32),
            pltpu.VMEM((seqs * 8, 128), f32),
            pltpu.VMEM((seqs * 4, 128), f32),
            pltpu.VMEM((seqs * 64, 256), bf16),
            pltpu.VMEM((kv_cache.shape[1], 256), f32),
            pltpu.VMEM((128, kv_cache.shape[1]), bf16),
            pltpu.VMEM((seqs * 4, 128), f32),
            pltpu.SemaphoreType.DMA((10,)),
            pltpu.SemaphoreType.DMA((kv_cache.shape[1] // SPAN,)),
        ],
        compiler_params=pltpu.CompilerParams(vmem_limit_bytes=24 * 1024 * 1024),
        name="attend",
    )(
        *in_hbm(
            lengths,
            lambdas,
            tokens,
            gain.reshape(1, -1),
            w_query,
            w_key.T,
            w_value.T,
            head_gain.reshape(1, -1),
            routing.T,
            route_weights.T,
            kv_cache,
        )
    )


def expert_kernel(
    rows,
    own_heads,
    heads_1,
    heads_2,
    heads_3,
    tokens,
    ffn_gain,
    w_gate,
    w_shared_gate,
    w_shared_up,
    w_out_hbm,
    w_up_hbm,
    w_down_hbm,
    w_shared_down_hbm,
    results,
    base,
    part_1,
    part_2,
    part_3,
    heads,
    partial,
    resid,
    w_out,
    w_up,
    w_down,
    w_shared_down,
    sems,
):
    slots = rows.shape[1]
    cuts = [pl.ds(256 * t, 256) for t in range(4)]
    loads = [(w_out_hbm.at[cut], w_out.at[cut]) for cut in cuts]
    loads += [(w_up_hbm.at[0], w_up), (w_down_hbm.at[0], w_down)]
    loads += [(w_shared_down_hbm, w_shared_down)]
    loads = [
        pltpu.make_async_copy(source, target, sems.at[i])
        for i, (source, target) in enumerate(loads)
    ]
    for load in loads:
        load.start()
    tp = lax.axis_index("tp")
    heads[tp] = own_heads[...]
    for k, got in enumerate((heads_1, heads_2, heads_3)):
        heads[(tp + 3 - k) % 4] = got[...]
    total = None
    for t in range(4):
        arrived = jnp.concatenate([rows[6 * t], rows[6 * t + 1]], axis=1)
        both = jnp.concatenate([arrived, heads[t]], axis=0)
        loads[t].wait()
        piece = jnp.dot(
            both, w_out[256 * t : 256 * t + 256, :], preferred_element_type=jnp.float32
        )
        piece = piece.astype(jnp.bfloat16).astype(jnp.float32)
        total = piece if total is None else total + piece
    row_tokens = jnp.concatenate([rows[6 * t + b] for t in range(4) for b in range(2, 6)], axis=1)
    all_tokens = jnp.concatenate([row_tokens, tokens[...]], axis=0)
    residual = (all_tokens.astype(jnp.float32) + total).astype(jnp.bfloat16)
    resid[...] = residual[slots:]
    wide = residual.astype(jnp.float32)
    scale = lax.rsqrt(jnp.mean(wide * wide, axis=1, keepdims=True) + epsilon)
    ffn_in = (wide * scale * ffn_gain[...]).astype(jnp.bfloat16)

    def gated(value, gate, up):
        gate_part = jnp.dot(value, gate, preferred_element_type=jnp.float32)
        up_part = jnp.dot(value, up, preferred_element_type=jnp.float32)
        return (gate_part / (1.0 + jnp.exp(-gate_part)) * up_part).astype(jnp.bfloat16)

    loads[4].wait()
    act = gated(ffn_in[:slots], w_gate[0], w_up[...])
    shared_act = gated(ffn_in[slots:], w_shared_gate[...], w_shared_up[...])
    loads[5].wait()
    result = jnp.dot(act, w_down[...], preferred_element_type=jnp.float32).astype(jnp.bfloat16)
    for b in range(16):
        results[b] = result[:, 128 * b : 128 * b + 128]
    loads[6].wait()
    partial[...] = jnp.dot(shared_act, w_shared_down[...], preferred_element_type=jnp.float32)

    def share(source, shift):
        at = pl.multiple_of(((tp + shift) % 4) * 512, 512)
        return source[:, pl.ds(at, 512)]

    base[...] = share(partial, 0) + share(resid, 0).astype(jnp.float32)
    for k, part in enumerate((part_1, part_2, part_3)):
        part[...] = share(partial, k + 1).astype(jnp.bfloat16)


def run_experts(rows, own_heads, got_heads, tokens, ffn_gain, weights):
    w_out, w_gate, w_up, w_down, w_shared_gate, w_shared_up, w_shared_down = weights
    seqs, width = tokens.shape
    vmem = pl.BlockSpec(memory_space=pltpu.VMEM)
    bf16, f32 = jnp.bfloat16, jnp.float32
    part = jax.ShapeDtypeStruct((seqs, 512), bf16)
    return pl.pallas_call(
        expert_kernel,
        out_shape=(
            jax.ShapeDtypeStruct((16, 64, 128), bf16),
            jax.ShapeDtypeStruct((seqs, 512), f32),
            part,
            part,
            part,
        ),
        in_specs=[vmem] * 10 + [pl.BlockSpec(memory_space=pltpu.HBM)] * 4,
        out_specs=(vmem,) * 5,
        scratch_shapes=[
            pltpu.VMEM((4, seqs, 256), bf16),
            pltpu.VMEM((seqs, width), f32),
            pltpu.VMEM((seqs, width), bf16),
            pltpu.VMEM(w_out.shape, bf16),
            pltpu.VMEM(w_up.shape[1:], bf16),
            pltpu.VMEM(w_down.shape[1:], bf16),
            pltpu.VMEM(w_shared_down.shape, bf16),
            pltpu.SemaphoreType.DMA((7,)),
        ],
        compiler_params=pltpu.CompilerParams(vmem_limit_bytes=24 * 1024 * 1024),
        name="run_experts",
    )(
        rows,
        own_heads,
        *got_heads,
        tokens,
        ffn_gain.reshape(1, -1),
        w_gate,
        w_shared_gate,
        w_shared_up,
        *in_hbm(w_out, w_up, w_down, w_shared_down),
    )


def finish_kernel(combine, returned, base, part_1, part_2, part_3, mixed):
    seqs = base.shape[0]
    total = base[...]
    for part in (part_1, part_2, part_3):
        total = total + part[...].astype(jnp.float32)
    arrived = jnp.concatenate([returned[b] for b in range(4)], axis=1)
    routed = jnp.dot(combine[...], arrived, preferred_element_type=jnp.float32)
    for k in range(3):
        total = total + routed[k * seqs : (k + 1) * seqs, :]
    mixed[...] = total.astype(jnp.bfloat16)


def finish(combine, returned, base, parts):
    vmem = pl.BlockSpec(memory_space=pltpu.VMEM)
    return pl.pallas_call(
        finish_kernel,
        out_shape=jax.ShapeDtypeStruct(base.shape, jnp.bfloat16),
        in_specs=[vmem] * 6,
        out_specs=vmem,
        compiler_params=pltpu.CompilerParams(vmem_limit_bytes=4 * 1024 * 1024),
        name="finish",
    )(combine, returned, base, *parts)


def around(value, shift):
    count = lax.axis_size("tp")
    return lax.ppermute(value, "tp", [(i, (i + shift) % count) for i in range(count)])


def shards(
    tokens,
    kv_cache,
    lengths,
    attn_gain,
    w_query,
    w_key,
    w_value,
    lambdas,
    head_gain,
    w_out,
    ffn_gain,
    w_shared_gate,
    w_shared_up,
    w_shared_down,
    routing,
    route_weights,
    w_exp_gate,
    w_exp_up,
    w_exp_down,
):
    everyone = ("ep", "tp")
    message, heads, combine = attend(
        tokens,
        kv_cache,
        lengths,
        attn_gain,
        w_query,
        w_key,
        w_value,
        lambdas,
        head_gain,
        routing,
        route_weights,
    )
    message = message.reshape(6, 128, 2, 128).transpose(1, 0, 2, 3)
    arrived = lax.all_to_all(message, everyone, split_axis=0, concat_axis=0, tiled=True)
    got_heads = [around(heads, k) for k in range(1, 4)]
    rows = arrived.reshape(32, 4, 6, 2, 128).transpose(1, 2, 0, 3, 4).reshape(24, 64, 128)
    results, base, *parts = run_experts(
        rows,
        heads,
        got_heads,
        tokens,
        ffn_gain,
        (w_out, w_exp_gate, w_exp_up, w_exp_down, w_shared_gate, w_shared_up, w_shared_down),
    )
    results = results.reshape(4, 4, 32, 2, 128).transpose(2, 0, 1, 3, 4)
    results = results.reshape(128, 4, 2, 128)
    returned = lax.all_to_all(results, everyone, split_axis=0, concat_axis=0, tiled=True)
    parts = [around(part, k + 1) for k, part in enumerate(parts)]
    returned = returned.transpose(1, 0, 2, 3).reshape(4, 256, 128)
    return finish(combine, returned, base, parts)


def solution(mesh):
    return jax.shard_map(
        shards,
        mesh=mesh,
        in_specs=(
            P("ep", None),
            P("ep", None, "tp"),
            P("ep"),
            P(),
            P(None, "tp"),
            P(None, "tp"),
            P(None, "tp"),
            P("tp"),
            P(),
            P(),
            P(),
            P(None, "tp"),
            P(None, "tp"),
            P("tp", None),
            P(),
            P("ep", None),
            P(("ep", "tp"), None, None),
            P(("ep", "tp"), None, None),
            P(("ep", "tp"), None, None),
        ),
        out_specs=P("ep", "tp"),
        check_vma=False,
    )
```

```python
import jax
import jax.numpy as jnp
from jax import lax
from jax.experimental import pallas as pl
from jax.experimental.pallas import tpu as pltpu
from jax.sharding import PartitionSpec as P

epsilon = 1e-06
neg_fill = -1e30
SPAN = 512
VMEM_BYTES = 64 * 1024 * 1024 - 65536


def attend_kernel(
    lengths_hbm,
    lambdas_hbm,
    tokens_hbm,
    gain_hbm,
    w_query_hbm,
    w_key_hbm,
    w_value_hbm,
    head_gain_hbm,
    routing_hbm,
    route_weights_hbm,
    kv_hbm,
    message,
    heads_out,
    combine_out,
    kv,
    lengths,
    lambdas,
    tokens,
    gain,
    w_query,
    w_key,
    w_value,
    head_gain,
    routing,
    route_weights,
    q8,
    n4,
    spread,
    scores,
    turned,
    mix,
    heads,
    combine,
    stage,
    ready,
    sems,
    kv_sems,
    send_sems,
):
    seqs, _ = tokens.shape
    cache_len = kv.shape[1]
    place = (lax.axis_index("ep"), lax.axis_index("tp"))
    spans = cache_len // SPAN
    rows_all = seqs * 4

    def kv_copy(i):
        part = pl.ds(i * SPAN, SPAN)
        return pltpu.make_async_copy(kv_hbm.at[:, part], kv.at[:, part], kv_sems.at[i])

    base = pl.multiple_of((place[0] // 4) * 128, 128)
    loads = [
        pltpu.make_async_copy(src, dst, sems.at[i])
        for i, (src, dst) in enumerate(
            [
                (tokens_hbm, tokens),
                (gain_hbm, gain),
                (w_query_hbm, w_query),
                (w_key_hbm, w_key),
                (w_value_hbm, w_value),
                (head_gain_hbm, head_gain),
                (routing_hbm.at[:, pl.ds(base, 128)], routing),
                (route_weights_hbm, route_weights),
                (lengths_hbm, lengths),
                (lambdas_hbm, lambdas),
            ]
        )
    ]
    for load in loads:
        load.start()
    for i in range(spans):
        kv_copy(i).start()

    lane = lax.broadcasted_iota(jnp.int32, (1, 128), 1)
    loads[0].wait()
    loads[1].wait()
    wide = tokens[...].astype(jnp.float32)
    scale = lax.rsqrt(jnp.mean(wide * wide, axis=1, keepdims=True) + epsilon)
    normed = (wide * scale * gain[...]).astype(jnp.bfloat16)
    for load in loads[2:]:
        load.wait()

    def rounded(value):
        return value.astype(jnp.bfloat16).astype(jnp.float32)

    def against(weight):
        return rounded(
            lax.dot_general(
                normed,
                weight[...],
                (((1,), (1,)), ((), ())),
                preferred_element_type=jnp.float32,
            )
        )

    queries = rounded(jnp.dot(normed, w_query[...], preferred_element_type=jnp.float32))
    new_row = jnp.concatenate([against(w_key), against(w_value)], axis=1)
    for head in range(4):
        pair = queries[:, 128 * (head // 2) : 128 * (head // 2) + 128]
        if head % 2:
            pair = pltpu.roll(pair, 64, 1)
        for half in range(2):
            own = (lane >= 32 * half) & (lane < 32 * half + 32)
            q8[pl.ds(half * rows_all + head, seqs, stride=4), :] = jnp.where(own, pair, 0.0)
        n4[pl.ds(head, seqs, stride=4), :] = new_row
    query_t = [q8[half * rows_all : (half + 1) * rows_all, :].T for half in range(2)]
    fresh = n4[...]
    fresh_t = fresh.T
    lane_seq = lax.broadcasted_iota(jnp.int32, (64, 128), 1) // 4
    for half in range(2):
        for s in range(seqs):
            spread[s * 64 : (s + 1) * 64, half * 128 : half * 128 + 128] = jnp.where(
                lane_seq == s, query_t[half][:64], 0.0
            ).astype(jnp.bfloat16)

    shift = 128 - (place[0] % 4) * 32
    named = jnp.where(lane < seqs, pltpu.roll(routing[...], shift, 1), -1)
    at_row = lax.broadcasted_iota(jnp.int32, (128, 128), 0)
    at_column = lax.broadcasted_iota(jnp.int32, (128, 128), 1)
    named_at = [at_row == named[k : k + 1, :] for k in range(4)]
    any_at = named_at[0] | named_at[1] | named_at[2] | named_at[3]
    before = (at_row < at_column).astype(jnp.float32).astype(jnp.bfloat16)
    rank = jnp.dot(
        any_at.astype(jnp.float32).astype(jnp.bfloat16),
        before,
        preferred_element_type=jnp.float32,
    )
    amount = jnp.zeros((128, 128), jnp.float32)
    widths = jnp.concatenate([route_weights[...]] * 4, axis=1)
    for k in range(4):
        amount = jnp.where(named_at[k], widths[k : k + 1, :], amount)
    picks = []
    for c in range(2):
        taken = any_at & (rank == float(c))
        picks.append(jnp.where(taken, 1.0, 0.0).astype(jnp.bfloat16)[:, :seqs])
        own_amount = jnp.where(taken, amount, 0.0).T[:seqs, :]
        for k in range(3):
            term = own_amount.astype(jnp.bfloat16)
            combine[k * seqs : (k + 1) * seqs, 128 * c : 128 * c + 128] = term
            own_amount = own_amount - term.astype(jnp.float32)

    def place_rows(source, first):
        for c in range(2):
            packed = jnp.dot(picks[c], source, preferred_element_type=jnp.float32)
            for b in range(source.shape[1] // 128):
                row = 2 * (first + b) + c
                stage[pl.ds(row, 128, stride=12), :] = packed[:, 128 * b : 128 * b + 128]

    share = tokens[:, pl.ds(pl.multiple_of(place[1] * 512, 128), 512)]
    place_rows(share, 2)

    scaling = 32 ** (-0.5)
    count = jnp.zeros((1, 128), jnp.int32)
    for s in range(seqs):
        count = jnp.where(lane // 4 == s, lengths[s], count)
    count = jnp.concatenate([count, count], axis=1)
    lam = jnp.zeros((1, 128), jnp.float32)
    for head in range(4):
        lam = jnp.where(lane % 4 == head, lambdas[head], lam)
    score_new = [
        jnp.sum(query_t[half] * fresh_t, axis=0, keepdims=True) * scaling for half in range(2)
    ]
    score_new = jnp.concatenate(score_new, axis=1)

    position = lax.broadcasted_iota(jnp.int32, (SPAN, 256), 0)
    highest = score_new
    for i in range(spans):
        kv_copy(i).wait()
        cut = slice(i * SPAN, (i + 1) * SPAN)
        part = jnp.concatenate([kv[s, cut, :64] for s in range(seqs)], axis=1)
        found = jnp.dot(part, spread[...], preferred_element_type=jnp.float32) * scaling
        found = jnp.where(position < count - i * SPAN, found, neg_fill)
        scores[i * SPAN : (i + 1) * SPAN, :] = found
        highest = jnp.maximum(highest, jnp.max(found, axis=0, keepdims=True))
    expo_new = jnp.exp(score_new - highest)
    total = expo_new
    for i in range(spans):
        found = scores[i * SPAN : (i + 1) * SPAN, :]
        expo = jnp.where(position < count - i * SPAN, jnp.exp(found - highest), 0.0)
        scores[i * SPAN : (i + 1) * SPAN, :] = expo
        total = total + jnp.sum(expo, axis=0, keepdims=True)
    factor = 1.0 / total
    first = factor[:, :128]
    second = lam * factor[:, 128:]
    for i in range(cache_len // 128):
        expo = scores[i * 128 : (i + 1) * 128, :]
        weight = expo[:, :128] * first - expo[:, 128:] * second
        turned[:, i * 128 : (i + 1) * 128] = weight.T.astype(jnp.bfloat16)
    weight_new = expo_new[:, :128] * first - expo_new[:, 128:] * second
    diagonal = jnp.where(at_row == at_column, weight_new, 0.0).astype(jnp.bfloat16)
    mix_new = jnp.dot(diagonal, fresh.astype(jnp.bfloat16), preferred_element_type=jnp.float32)
    upper = lax.broadcasted_iota(jnp.int32, (8, 1), 0) < 4
    for i in range(seqs // 2):
        both = jnp.concatenate([kv[2 * i], kv[2 * i + 1]], axis=1)
        out = jnp.dot(turned[8 * i : 8 * i + 8, :], both, preferred_element_type=jnp.float32)
        mix[8 * i : 8 * i + 8, :] = jnp.where(upper, out[:, :128], out[:, 128:])

    blend = mix[...] + mix_new
    values = jnp.where(lane >= 64, blend, 0.0)
    power = jnp.sum(values * values, axis=1, keepdims=True) * (1.0 / 64)
    gain2 = jnp.concatenate([head_gain[...], head_gain[...]], axis=1)
    mix[...] = blend * lax.rsqrt(power + epsilon) * gain2
    pieces = []
    for pair in range(2):
        even = mix[pl.ds(2 * pair, seqs, stride=4), :]
        odd = mix[pl.ds(2 * pair + 1, seqs, stride=4), :]
        both = jnp.where(lane < 64, pltpu.roll(even, 64, 1), odd).astype(jnp.bfloat16)
        heads[:, 128 * pair : 128 * pair + 128] = both
        pieces.append(both)
    extra = [
        pltpu.make_async_copy(heads, heads_out, send_sems.at[4]),
        pltpu.make_async_copy(combine, combine_out, send_sems.at[5]),
    ]
    for send in extra:
        send.start()
    place_rows(jnp.concatenate(pieces, axis=1), 0)
    sends = []
    for i in range(4):
        part = pl.ds(384 * i, 384)
        ready[part, :] = stage[part, :].astype(jnp.bfloat16)
        sends.append(
            pltpu.make_async_copy(ready.at[part], message.at[part], send_sems.at[i])
        )
        sends[i].start()
    for send in sends + extra:
        send.wait()


def in_hbm(*arrays):
    return [pltpu.with_memory_space_constraint(array, pltpu.HBM) for array in arrays]


def attend(
    tokens, kv_cache, lengths, gain, w_query, w_key, w_value, lambdas, head_gain, routing,
    route_weights,
):
    seqs, width = tokens.shape
    hbm = pl.BlockSpec(memory_space=pltpu.HBM)
    bf16, f32 = jnp.bfloat16, jnp.float32
    return pl.pallas_call(
        attend_kernel,
        out_shape=(
            pltpu.HBM((1536, 128), bf16),
            pltpu.HBM((seqs, 256), bf16),
            pltpu.HBM((3 * seqs, 256), bf16),
        ),
        in_specs=[hbm] * 11,
        out_specs=(hbm, hbm, hbm),
        scratch_shapes=[
            pltpu.VMEM(kv_cache.shape, bf16),
            pltpu.SMEM((seqs,), jnp.int32),
            pltpu.SMEM((4,), f32),
            pltpu.VMEM((seqs, width), bf16),
            pltpu.VMEM((1, width), f32),
            pltpu.VMEM((width, 256), bf16),
            pltpu.VMEM((64, width), bf16),
            pltpu.VMEM((64, width), bf16),
            pltpu.VMEM((1, 64), f32),
            pltpu.VMEM((4, 128), jnp.int32),
            pltpu.VMEM((4, seqs), f32),
            pltpu.VMEM((seqs * 8, 128), f32),
            pltpu.VMEM((seqs * 4, 128), f32),
            pltpu.VMEM((seqs * 64, 256), bf16),
            pltpu.VMEM((kv_cache.shape[1], 256), f32),
            pltpu.VMEM((128, kv_cache.shape[1]), bf16),
            pltpu.VMEM((seqs * 4, 128), f32),
            pltpu.VMEM((seqs, 256), bf16),
            pltpu.VMEM((3 * seqs, 256), bf16),
            pltpu.VMEM((1536, 128), f32),
            pltpu.VMEM((1536, 128), bf16),
            pltpu.SemaphoreType.DMA((10,)),
            pltpu.SemaphoreType.DMA((kv_cache.shape[1] // SPAN,)),
            pltpu.SemaphoreType.DMA((6,)),
        ],
        compiler_params=pltpu.CompilerParams(vmem_limit_bytes=VMEM_BYTES),
        name="attend",
    )(
        *in_hbm(
            lengths,
            lambdas,
            tokens,
            gain.reshape(1, -1),
            w_query,
            w_key.T,
            w_value.T,
            head_gain.reshape(1, -1),
            routing.T,
            route_weights.T,
            kv_cache,
        )
    )


def expert_kernel(
    rows,
    own_heads,
    heads_1,
    heads_2,
    heads_3,
    tokens_hbm,
    ffn_gain_hbm,
    w_out_hbm,
    w_gate_hbm,
    w_up_hbm,
    w_down_hbm,
    w_shared_gate_hbm,
    w_shared_up_hbm,
    w_shared_down_hbm,
    results,
    base_out,
    part_1,
    part_2,
    part_3,
    heads,
    base,
    parts,
    partial,
    resid,
    wide_rows,
    stage,
    ready,
    tokens,
    ffn_gain,
    w_out,
    w_gate,
    w_up,
    w_down,
    w_shared_gate,
    w_shared_up,
    w_shared_down,
    sems,
    head_sems,
    send_sems,
):
    slots = 64
    quarters = [pl.ds(256 * t, 256) for t in range(4)]
    tp = lax.axis_index("tp")
    loads = [(w_out_hbm.at[quarter], w_out.at[quarter]) for quarter in quarters]
    gathered = [(own_heads, heads.at[tp])]
    for k, got in enumerate((heads_1, heads_2, heads_3)):
        gathered.append((got, heads.at[(tp + 3 - k) % 4]))
    gathered = [
        pltpu.make_async_copy(source, target, head_sems.at[i])
        for i, (source, target) in enumerate(gathered)
    ]
    for load in gathered:
        load.start()
    loads += [(tokens_hbm, tokens), (ffn_gain_hbm, ffn_gain)]
    loads += [(w_gate_hbm.at[0], w_gate), (w_up_hbm.at[0], w_up)]
    loads += [(w_shared_gate_hbm, w_shared_gate), (w_shared_up_hbm, w_shared_up)]
    loads += [(w_down_hbm.at[0], w_down), (w_shared_down_hbm, w_shared_down)]
    loads = [
        pltpu.make_async_copy(source, target, sems.at[i])
        for i, (source, target) in enumerate(loads)
    ]
    for load in loads:
        load.start()
    wide_rows[...] = rows[...].astype(jnp.float32)

    def arrived_rows(t, b):
        halves = [
            wide_rows[pl.ds(12 * t + 2 * b + c, 32, stride=48), :].astype(jnp.bfloat16)
            for c in range(2)
        ]
        return jnp.concatenate(halves, axis=0)

    for load in gathered:
        load.wait()
    total = None
    for t in range(4):
        arrived = jnp.concatenate([arrived_rows(t, 0), arrived_rows(t, 1)], axis=1)
        both = jnp.concatenate([arrived, heads[t]], axis=0)
        loads[t].wait()
        piece = jnp.dot(
            both, w_out[256 * t : 256 * t + 256, :], preferred_element_type=jnp.float32
        )
        piece = piece.astype(jnp.bfloat16).astype(jnp.float32)
        total = piece if total is None else total + piece
    row_tokens = jnp.concatenate([arrived_rows(t, b) for t in range(4) for b in range(2, 6)], axis=1)
    loads[4].wait()
    loads[5].wait()
    all_tokens = jnp.concatenate([row_tokens, tokens[...]], axis=0)
    residual = (all_tokens.astype(jnp.float32) + total).astype(jnp.bfloat16)
    resid[...] = residual[slots:]
    wide = residual.astype(jnp.float32)
    scale = lax.rsqrt(jnp.mean(wide * wide, axis=1, keepdims=True) + epsilon)
    ffn_in = (wide * scale * ffn_gain[...]).astype(jnp.bfloat16)

    def gated(value, gate, up):
        gate_part = jnp.dot(value, gate, preferred_element_type=jnp.float32)
        up_part = jnp.dot(value, up, preferred_element_type=jnp.float32)
        return (gate_part / (1.0 + jnp.exp(-gate_part)) * up_part).astype(jnp.bfloat16)

    loads[6].wait()
    loads[7].wait()
    act = gated(ffn_in[:slots], w_gate[...], w_up[...])
    loads[8].wait()
    loads[9].wait()
    shared_act = gated(ffn_in[slots:], w_shared_gate[...], w_shared_up[...])
    loads[10].wait()
    result = jnp.dot(act, w_down[...], preferred_element_type=jnp.float32)
    for b in range(16):
        for c in range(2):
            stage[pl.ds(2 * b + c, 32, stride=32), :] = result[
                32 * c : 32 * c + 32, 128 * b : 128 * b + 128
            ]
    sends = []
    for i in range(2):
        half = pl.ds(512 * i, 512)
        ready[half, :] = stage[half, :].astype(jnp.bfloat16)
        sends.append(
            pltpu.make_async_copy(ready.at[half], results.at[half], send_sems.at[i])
        )
        sends[i].start()
    loads[11].wait()
    partial[...] = jnp.dot(shared_act, w_shared_down[...], preferred_element_type=jnp.float32)

    def share(source, shift):
        at = pl.multiple_of(((tp + shift) % 4) * 512, 512)
        return source[:, pl.ds(at, 512)]

    base[...] = share(partial, 0) + share(resid, 0).astype(jnp.float32)
    sends.append(pltpu.make_async_copy(base, base_out, send_sems.at[2]))
    sends[2].start()
    for k, part in enumerate((part_1, part_2, part_3)):
        parts[k] = share(partial, k + 1).astype(jnp.bfloat16)
        sends.append(pltpu.make_async_copy(parts.at[k], part, send_sems.at[3 + k]))
        sends[3 + k].start()
    for send in sends:
        send.wait()


def run_experts(rows, own_heads, got_heads, tokens, ffn_gain, weights):
    w_out, w_gate, w_up, w_down, w_shared_gate, w_shared_up, w_shared_down = weights
    seqs, width = tokens.shape
    vmem = pl.BlockSpec(memory_space=pltpu.VMEM)
    bf16, f32 = jnp.bfloat16, jnp.float32
    part = pltpu.HBM((seqs, 512), bf16)
    hbm = pl.BlockSpec(memory_space=pltpu.HBM)
    either = pl.BlockSpec(memory_space=pl.ANY)
    return pl.pallas_call(
        expert_kernel,
        out_shape=(
            pltpu.HBM((1024, 128), bf16),
            pltpu.HBM((seqs, 512), f32),
            part,
            part,
            part,
        ),
        in_specs=[vmem] + [either] * 4 + [hbm] * 9,
        out_specs=(hbm,) * 5,
        scratch_shapes=[
            pltpu.VMEM((4, seqs, 256), bf16),
            pltpu.VMEM((seqs, 512), f32),
            pltpu.VMEM((3, seqs, 512), bf16),
            pltpu.VMEM((seqs, width), f32),
            pltpu.VMEM((seqs, width), bf16),
            pltpu.VMEM((1536, 128), f32),
            pltpu.VMEM((1024, 128), f32),
            pltpu.VMEM((1024, 128), bf16),
            pltpu.VMEM((seqs, width), bf16),
            pltpu.VMEM((1, width), f32),
            pltpu.VMEM(w_out.shape, bf16),
            pltpu.VMEM(w_gate.shape[1:], bf16),
            pltpu.VMEM(w_up.shape[1:], bf16),
            pltpu.VMEM(w_down.shape[1:], bf16),
            pltpu.VMEM(w_shared_gate.shape, bf16),
            pltpu.VMEM(w_shared_up.shape, bf16),
            pltpu.VMEM(w_shared_down.shape, bf16),
            pltpu.SemaphoreType.DMA((12,)),
            pltpu.SemaphoreType.DMA((4,)),
            pltpu.SemaphoreType.DMA((6,)),
        ],
        compiler_params=pltpu.CompilerParams(vmem_limit_bytes=24 * 1024 * 1024),
        name="run_experts",
    )(
        rows,
        *in_hbm(own_heads),
        *got_heads,
        *in_hbm(tokens, ffn_gain.reshape(1, -1), *weights),
    )


def finish_kernel(
    returned,
    combine_any,
    base_any,
    part_1,
    part_2,
    part_3,
    mixed,
    wide,
    combine,
    base,
    parts,
    sems,
):
    seqs = base.shape[0]
    loads = [(combine_any, combine), (base_any, base)]
    loads += [(part, parts.at[k]) for k, part in enumerate((part_1, part_2, part_3))]
    loads = [
        pltpu.make_async_copy(source, target, sems.at[i])
        for i, (source, target) in enumerate(loads)
    ]
    for load in loads:
        load.start()
    wide[...] = returned[...].astype(jnp.float32)
    arrived = jnp.concatenate(
        [
            jnp.concatenate(
                [
                    wide[pl.ds(2 * b + c, 128, stride=8), :].astype(jnp.bfloat16)
                    for b in range(4)
                ],
                axis=1,
            )
            for c in range(2)
        ],
        axis=0,
    )
    for load in loads:
        load.wait()
    routed = jnp.dot(combine[...], arrived, preferred_element_type=jnp.float32)
    total = base[...]
    for k in range(3):
        total = total + parts[k].astype(jnp.float32)
    for k in range(3):
        total = total + routed[k * seqs : (k + 1) * seqs, :]
    mixed[...] = total.astype(jnp.bfloat16)


def finish(combine, returned, base, parts):
    vmem = pl.BlockSpec(memory_space=pltpu.VMEM)
    return pl.pallas_call(
        finish_kernel,
        out_shape=jax.ShapeDtypeStruct(base.shape, jnp.bfloat16),
        in_specs=[vmem] + [pl.BlockSpec(memory_space=pl.ANY)] * 5,
        out_specs=vmem,
        scratch_shapes=[
            pltpu.VMEM((1024, 128), jnp.float32),
            pltpu.VMEM(combine.shape, jnp.bfloat16),
            pltpu.VMEM(base.shape, jnp.float32),
            pltpu.VMEM((3, *base.shape), jnp.bfloat16),
            pltpu.SemaphoreType.DMA((5,)),
        ],
        compiler_params=pltpu.CompilerParams(vmem_limit_bytes=4 * 1024 * 1024),
        name="finish",
    )(returned, *in_hbm(combine, base), *parts)


def around(value, shift):
    count = lax.axis_size("tp")
    return lax.ppermute(value, "tp", [(i, (i + shift) % count) for i in range(count)])


def shards(
    tokens,
    kv_cache,
    lengths,
    attn_gain,
    w_query,
    w_key,
    w_value,
    lambdas,
    head_gain,
    w_out,
    ffn_gain,
    w_shared_gate,
    w_shared_up,
    w_shared_down,
    routing,
    route_weights,
    w_exp_gate,
    w_exp_up,
    w_exp_down,
):
    everyone = ("ep", "tp")
    message, heads, combine = attend(
        tokens,
        kv_cache,
        lengths,
        attn_gain,
        w_query,
        w_key,
        w_value,
        lambdas,
        head_gain,
        routing,
        route_weights,
    )
    message = message.reshape(128, 6, 2, 128)
    arrived = lax.all_to_all(message, everyone, split_axis=0, concat_axis=0, tiled=True)
    got_heads = [around(heads, k) for k in range(1, 4)]
    rows = arrived.reshape(1536, 128)
    results, base, *parts = run_experts(
        rows,
        heads,
        got_heads,
        tokens,
        ffn_gain,
        (
            w_out,
            w_exp_gate,
            w_exp_up,
            w_exp_down,
            w_shared_gate,
            w_shared_up,
            w_shared_down,
        ),
    )
    results = results.reshape(128, 4, 2, 128)
    returned = lax.all_to_all(results, everyone, split_axis=0, concat_axis=0, tiled=True)
    parts = [around(part, k + 1) for k, part in enumerate(parts)]
    returned = returned.reshape(1024, 128)
    return finish(combine, returned, base, parts)


def solution(mesh):
    return jax.shard_map(
        shards,
        mesh=mesh,
        in_specs=(
            P("ep", None),
            P("ep", None, "tp"),
            P("ep"),
            P(),
            P(None, "tp"),
            P(None, "tp"),
            P(None, "tp"),
            P("tp"),
            P(),
            P(),
            P(),
            P(None, "tp"),
            P(None, "tp"),
            P("tp", None),
            P(),
            P("ep", None),
            P(("ep", "tp"), None, None),
            P(("ep", "tp"), None, None),
            P(("ep", "tp"), None, None),
        ),
        out_specs=P("ep", "tp"),
        check_vma=False,
    )
```

```python
import jax
import jax.numpy as jnp
from jax import lax
from jax.experimental import pallas as pl
from jax.experimental.pallas import tpu as pltpu
from jax.sharding import PartitionSpec as P

epsilon = 1e-06
neg_fill = -1e30
SPAN = 512
VMEM_BYTES = 64 * 1024 * 1024 - 65536


def attend_kernel(
    lengths_hbm,
    lambdas_hbm,
    tokens_hbm,
    gain_hbm,
    w_query_hbm,
    w_key_hbm,
    w_value_hbm,
    head_gain_hbm,
    routing_hbm,
    route_weights_hbm,
    kv_hbm,
    message,
    heads_out,
    combine_out,
    kv,
    lengths,
    lambdas,
    tokens,
    gain,
    w_query,
    w_key,
    w_value,
    head_gain,
    routing,
    route_weights,
    q8,
    n4,
    spread,
    scores,
    turned,
    mix,
    heads,
    combine,
    stage,
    ready,
    sems,
    kv_sems,
    send_sems,
):
    seqs, _ = tokens.shape
    cache_len = kv.shape[1]
    place = (lax.axis_index("ep"), lax.axis_index("tp"))
    spans = cache_len // SPAN
    rows_all = seqs * 4

    def kv_copy(i):
        part = pl.ds(i * SPAN, SPAN)
        return pltpu.make_async_copy(kv_hbm.at[:, part], kv.at[:, part], kv_sems.at[i])

    base = pl.multiple_of((place[0] // 4) * 128, 128)
    loads = [
        pltpu.make_async_copy(src, dst, sems.at[i])
        for i, (src, dst) in enumerate(
            [
                (tokens_hbm, tokens),
                (gain_hbm, gain),
                (w_query_hbm, w_query),
                (w_key_hbm, w_key),
                (w_value_hbm, w_value),
                (head_gain_hbm, head_gain),
                (routing_hbm.at[:, pl.ds(base, 128)], routing),
                (route_weights_hbm, route_weights),
                (lengths_hbm, lengths),
                (lambdas_hbm, lambdas),
            ]
        )
    ]
    for load in loads:
        load.start()
    for i in range(spans):
        kv_copy(i).start()

    lane = lax.broadcasted_iota(jnp.int32, (1, 128), 1)
    loads[0].wait()
    loads[1].wait()
    wide = tokens[...].astype(jnp.float32)
    scale = lax.rsqrt(jnp.mean(wide * wide, axis=1, keepdims=True) + epsilon)
    normed = (wide * scale * gain[...]).astype(jnp.bfloat16)
    for load in loads[2:]:
        load.wait()

    def rounded(value):
        return value.astype(jnp.bfloat16).astype(jnp.float32)

    def against(weight):
        return rounded(
            lax.dot_general(
                normed,
                weight[...],
                (((1,), (1,)), ((), ())),
                preferred_element_type=jnp.float32,
            )
        )

    queries = rounded(jnp.dot(normed, w_query[...], preferred_element_type=jnp.float32))
    new_row = jnp.concatenate([against(w_key), against(w_value)], axis=1)
    for head in range(4):
        pair = queries[:, 128 * (head // 2) : 128 * (head // 2) + 128]
        if head % 2:
            pair = pltpu.roll(pair, 64, 1)
        for half in range(2):
            own = (lane >= 32 * half) & (lane < 32 * half + 32)
            q8[pl.ds(half * rows_all + head, seqs, stride=4), :] = jnp.where(own, pair, 0.0)
        n4[pl.ds(head, seqs, stride=4), :] = new_row
    query_t = [q8[half * rows_all : (half + 1) * rows_all, :].T for half in range(2)]
    fresh = n4[...]
    fresh_t = fresh.T
    lane_seq = lax.broadcasted_iota(jnp.int32, (64, 128), 1) // 4
    for half in range(2):
        for s in range(seqs):
            spread[s * 64 : (s + 1) * 64, half * 128 : half * 128 + 128] = jnp.where(
                lane_seq == s, query_t[half][:64], 0.0
            ).astype(jnp.bfloat16)

    shift = 128 - (place[0] % 4) * 32
    named = jnp.where(lane < seqs, pltpu.roll(routing[...], shift, 1), -1)
    at_row = lax.broadcasted_iota(jnp.int32, (128, 128), 0)
    at_column = lax.broadcasted_iota(jnp.int32, (128, 128), 1)
    named_at = [at_row == named[k : k + 1, :] for k in range(4)]
    any_at = named_at[0] | named_at[1] | named_at[2] | named_at[3]
    before = (at_row < at_column).astype(jnp.float32).astype(jnp.bfloat16)
    rank = jnp.dot(
        any_at.astype(jnp.float32).astype(jnp.bfloat16),
        before,
        preferred_element_type=jnp.float32,
    )
    amount = jnp.zeros((128, 128), jnp.float32)
    widths = jnp.concatenate([route_weights[...]] * 4, axis=1)
    for k in range(4):
        amount = jnp.where(named_at[k], widths[k : k + 1, :], amount)
    picks = []
    for c in range(2):
        taken = any_at & (rank == float(c))
        picks.append(jnp.where(taken, 1.0, 0.0).astype(jnp.bfloat16)[:, :seqs])
        own_amount = jnp.where(taken, amount, 0.0).T[:seqs, :]
        for k in range(3):
            term = own_amount.astype(jnp.bfloat16)
            combine[k * seqs : (k + 1) * seqs, 128 * c : 128 * c + 128] = term
            own_amount = own_amount - term.astype(jnp.float32)

    def place_rows(source, first):
        for c in range(2):
            packed = jnp.dot(picks[c], source, preferred_element_type=jnp.float32)
            for b in range(source.shape[1] // 128):
                row = 2 * (first + b) + c
                stage[pl.ds(row, 128, stride=12), :] = packed[:, 128 * b : 128 * b + 128]

    share = tokens[:, pl.ds(pl.multiple_of(place[1] * 512, 128), 512)]
    place_rows(share, 2)

    scaling = 32 ** (-0.5)
    count = jnp.zeros((1, 128), jnp.int32)
    for s in range(seqs):
        count = jnp.where(lane // 4 == s, lengths[s], count)
    count = jnp.concatenate([count, count], axis=1)
    lam = jnp.zeros((1, 128), jnp.float32)
    for head in range(4):
        lam = jnp.where(lane % 4 == head, lambdas[head], lam)
    score_new = [
        jnp.sum(query_t[half] * fresh_t, axis=0, keepdims=True) * scaling for half in range(2)
    ]
    score_new = jnp.concatenate(score_new, axis=1)

    position = lax.broadcasted_iota(jnp.int32, (SPAN, 256), 0)
    highest = score_new
    for i in range(spans):
        kv_copy(i).wait()
        cut = slice(i * SPAN, (i + 1) * SPAN)
        part = jnp.concatenate([kv[s, cut, :64] for s in range(seqs)], axis=1)
        found = jnp.dot(part, spread[...], preferred_element_type=jnp.float32) * scaling
        found = jnp.where(position < count - i * SPAN, found, neg_fill)
        scores[i * SPAN : (i + 1) * SPAN, :] = found
        highest = jnp.maximum(highest, jnp.max(found, axis=0, keepdims=True))
    expo_new = jnp.exp(score_new - highest)
    total = expo_new
    for i in range(spans):
        found = scores[i * SPAN : (i + 1) * SPAN, :]
        expo = jnp.where(position < count - i * SPAN, jnp.exp(found - highest), 0.0)
        scores[i * SPAN : (i + 1) * SPAN, :] = expo
        total = total + jnp.sum(expo, axis=0, keepdims=True)
    factor = 1.0 / total
    first = factor[:, :128]
    second = lam * factor[:, 128:]
    for i in range(cache_len // 128):
        expo = scores[i * 128 : (i + 1) * 128, :]
        weight = expo[:, :128] * first - expo[:, 128:] * second
        turned[:, i * 128 : (i + 1) * 128] = weight.T.astype(jnp.bfloat16)
    weight_new = expo_new[:, :128] * first - expo_new[:, 128:] * second
    diagonal = jnp.where(at_row == at_column, weight_new, 0.0).astype(jnp.bfloat16)
    mix_new = jnp.dot(diagonal, fresh.astype(jnp.bfloat16), preferred_element_type=jnp.float32)
    upper = lax.broadcasted_iota(jnp.int32, (8, 1), 0) < 4
    for i in range(seqs // 2):
        both = jnp.concatenate([kv[2 * i], kv[2 * i + 1]], axis=1)
        out = jnp.dot(turned[8 * i : 8 * i + 8, :], both, preferred_element_type=jnp.float32)
        mix[8 * i : 8 * i + 8, :] = jnp.where(upper, out[:, :128], out[:, 128:])

    blend = mix[...] + mix_new
    values = jnp.where(lane >= 64, blend, 0.0)
    power = jnp.sum(values * values, axis=1, keepdims=True) * (1.0 / 64)
    gain2 = jnp.concatenate([head_gain[...], head_gain[...]], axis=1)
    mix[...] = blend * lax.rsqrt(power + epsilon) * gain2
    pieces = []
    for pair in range(2):
        even = mix[pl.ds(2 * pair, seqs, stride=4), :]
        odd = mix[pl.ds(2 * pair + 1, seqs, stride=4), :]
        both = jnp.where(lane < 64, pltpu.roll(even, 64, 1), odd).astype(jnp.bfloat16)
        heads[:, 128 * pair : 128 * pair + 128] = both
        pieces.append(both)
    extra = [
        pltpu.make_async_copy(heads, heads_out, send_sems.at[4]),
        pltpu.make_async_copy(combine, combine_out, send_sems.at[5]),
    ]
    for send in extra:
        send.start()
    place_rows(jnp.concatenate(pieces, axis=1), 0)
    sends = []
    for i in range(4):
        part = pl.ds(384 * i, 384)
        ready[part, :] = stage[part, :].astype(jnp.bfloat16)
        sends.append(
            pltpu.make_async_copy(ready.at[part], message.at[part], send_sems.at[i])
        )
        sends[i].start()
    for send in sends + extra:
        send.wait()


def in_hbm(*arrays):
    return [pltpu.with_memory_space_constraint(array, pltpu.HBM) for array in arrays]


def attend(
    tokens, kv_cache, lengths, gain, w_query, w_key, w_value, lambdas, head_gain, routing,
    route_weights,
):
    seqs, width = tokens.shape
    hbm = pl.BlockSpec(memory_space=pltpu.HBM)
    bf16, f32 = jnp.bfloat16, jnp.float32
    return pl.pallas_call(
        attend_kernel,
        out_shape=(
            pltpu.HBM((1536, 128), bf16),
            pltpu.HBM((seqs, 256), bf16),
            pltpu.HBM((3 * seqs, 256), bf16),
        ),
        in_specs=[hbm] * 11,
        out_specs=(hbm, hbm, hbm),
        scratch_shapes=[
            pltpu.VMEM(kv_cache.shape, bf16),
            pltpu.SMEM((seqs,), jnp.int32),
            pltpu.SMEM((4,), f32),
            pltpu.VMEM((seqs, width), bf16),
            pltpu.VMEM((1, width), f32),
            pltpu.VMEM((width, 256), bf16),
            pltpu.VMEM((64, width), bf16),
            pltpu.VMEM((64, width), bf16),
            pltpu.VMEM((1, 64), f32),
            pltpu.VMEM((4, 128), jnp.int32),
            pltpu.VMEM((4, seqs), f32),
            pltpu.VMEM((seqs * 8, 128), f32),
            pltpu.VMEM((seqs * 4, 128), f32),
            pltpu.VMEM((seqs * 64, 256), bf16),
            pltpu.VMEM((kv_cache.shape[1], 256), f32),
            pltpu.VMEM((128, kv_cache.shape[1]), bf16),
            pltpu.VMEM((seqs * 4, 128), f32),
            pltpu.VMEM((seqs, 256), bf16),
            pltpu.VMEM((3 * seqs, 256), bf16),
            pltpu.VMEM((1536, 128), f32),
            pltpu.VMEM((1536, 128), bf16),
            pltpu.SemaphoreType.DMA((10,)),
            pltpu.SemaphoreType.DMA((kv_cache.shape[1] // SPAN,)),
            pltpu.SemaphoreType.DMA((6,)),
        ],
        compiler_params=pltpu.CompilerParams(vmem_limit_bytes=VMEM_BYTES),
        name="attend",
    )(
        *in_hbm(
            lengths,
            lambdas,
            tokens,
            gain.reshape(1, -1),
            w_query,
            w_key.T,
            w_value.T,
            head_gain.reshape(1, -1),
            routing.T,
            route_weights.T,
            kv_cache,
        )
    )


def fetch_kernel(after, *refs):
    count = (len(refs) - 1) // 2
    loads = [
        pltpu.make_async_copy(refs[i], refs[count + i], refs[-1].at[i]) for i in range(count)
    ]
    for load in loads:
        load.start()
    for load in loads:
        load.wait()


def fetch(after, arrays):
    hbm = pl.BlockSpec(memory_space=pltpu.HBM)
    return pl.pallas_call(
        fetch_kernel,
        out_shape=tuple(jax.ShapeDtypeStruct(a.shape, a.dtype) for a in arrays),
        in_specs=[hbm] * (1 + len(arrays)),
        out_specs=(pl.BlockSpec(memory_space=pltpu.VMEM),) * len(arrays),
        scratch_shapes=[pltpu.SemaphoreType.DMA((len(arrays),))],
        compiler_params=pltpu.CompilerParams(vmem_limit_bytes=1024 * 1024),
        name="fetch",
    )(*in_hbm(after, *arrays))


def expert_kernel(
    rows,
    w_gate,
    own_heads,
    heads_1,
    heads_2,
    heads_3,
    tokens_hbm,
    ffn_gain_hbm,
    w_out_hbm,
    w_up_hbm,
    w_down_hbm,
    w_shared_gate_hbm,
    w_shared_up_hbm,
    w_shared_down_hbm,
    results,
    base_out,
    part_1,
    part_2,
    part_3,
    heads,
    base,
    parts,
    partial,
    resid,
    wide_rows,
    stage,
    ready,
    tokens,
    ffn_gain,
    w_out,
    w_up,
    w_down,
    w_shared_gate,
    w_shared_up,
    w_shared_down,
    sems,
    head_sems,
    send_sems,
):
    slots = 64
    quarters = [pl.ds(256 * t, 256) for t in range(4)]
    tp = lax.axis_index("tp")
    loads = [(w_out_hbm.at[quarter], w_out.at[quarter]) for quarter in quarters]
    gathered = [(own_heads, heads.at[tp])]
    for k, got in enumerate((heads_1, heads_2, heads_3)):
        gathered.append((got, heads.at[(tp + 3 - k) % 4]))
    gathered = [
        pltpu.make_async_copy(source, target, head_sems.at[i])
        for i, (source, target) in enumerate(gathered)
    ]
    for load in gathered:
        load.start()
    loads += [(tokens_hbm, tokens), (ffn_gain_hbm, ffn_gain)]
    loads += [(w_up_hbm.at[0], w_up), (w_down_hbm.at[0], w_down)]
    loads += [(w_shared_gate_hbm, w_shared_gate), (w_shared_up_hbm, w_shared_up)]
    loads += [(w_shared_down_hbm, w_shared_down)]
    loads = [
        pltpu.make_async_copy(source, target, sems.at[i])
        for i, (source, target) in enumerate(loads)
    ]
    for load in loads:
        load.start()
    wide_rows[...] = rows[...].astype(jnp.float32)

    def arrived_rows(t, b):
        halves = [
            wide_rows[pl.ds(12 * t + 2 * b + c, 32, stride=48), :].astype(jnp.bfloat16)
            for c in range(2)
        ]
        return jnp.concatenate(halves, axis=0)

    for load in gathered:
        load.wait()
    total = None
    for t in range(4):
        arrived = jnp.concatenate([arrived_rows(t, 0), arrived_rows(t, 1)], axis=1)
        both = jnp.concatenate([arrived, heads[t]], axis=0)
        loads[t].wait()
        piece = jnp.dot(
            both, w_out[256 * t : 256 * t + 256, :], preferred_element_type=jnp.float32
        )
        piece = piece.astype(jnp.bfloat16).astype(jnp.float32)
        total = piece if total is None else total + piece
    row_tokens = jnp.concatenate([arrived_rows(t, b) for t in range(4) for b in range(2, 6)], axis=1)
    loads[4].wait()
    loads[5].wait()
    all_tokens = jnp.concatenate([row_tokens, tokens[...]], axis=0)
    residual = (all_tokens.astype(jnp.float32) + total).astype(jnp.bfloat16)
    resid[...] = residual[slots:]
    wide = residual.astype(jnp.float32)
    scale = lax.rsqrt(jnp.mean(wide * wide, axis=1, keepdims=True) + epsilon)
    ffn_in = (wide * scale * ffn_gain[...]).astype(jnp.bfloat16)

    def gated(value, gate, up):
        gate_part = jnp.dot(value, gate, preferred_element_type=jnp.float32)
        up_part = jnp.dot(value, up, preferred_element_type=jnp.float32)
        return (gate_part / (1.0 + jnp.exp(-gate_part)) * up_part).astype(jnp.bfloat16)

    loads[6].wait()
    act = gated(ffn_in[:slots], w_gate[0], w_up[...])
    loads[7].wait()
    result = jnp.dot(act, w_down[...], preferred_element_type=jnp.float32)
    for b in range(16):
        for c in range(2):
            stage[pl.ds(2 * b + c, 32, stride=32), :] = result[
                32 * c : 32 * c + 32, 128 * b : 128 * b + 128
            ]
    sends = []
    for i in range(2):
        half = pl.ds(512 * i, 512)
        ready[half, :] = stage[half, :].astype(jnp.bfloat16)
        sends.append(pltpu.make_async_copy(ready.at[half], results.at[half], send_sems.at[i]))
        sends[i].start()
    loads[8].wait()
    loads[9].wait()
    shared_act = gated(ffn_in[slots:], w_shared_gate[...], w_shared_up[...])
    loads[10].wait()
    partial[...] = jnp.dot(shared_act, w_shared_down[...], preferred_element_type=jnp.float32)

    def share(source, shift):
        at = pl.multiple_of(((tp + shift) % 4) * 512, 512)
        return source[:, pl.ds(at, 512)]

    for k, part in enumerate((part_1, part_2, part_3)):
        parts[k] = share(partial, k + 1).astype(jnp.bfloat16)
        sends.append(pltpu.make_async_copy(parts.at[k], part, send_sems.at[2 + k]))
        sends[2 + k].start()
    base[...] = share(partial, 0) + share(resid, 0).astype(jnp.float32)
    sends.append(pltpu.make_async_copy(base, base_out, send_sems.at[5]))
    sends[5].start()
    for send in sends:
        send.wait()


def run_experts(rows, own_heads, got_heads, tokens, ffn_gain, w_gate, weights):
    w_out, w_up, w_down, w_shared_gate, w_shared_up, w_shared_down = weights
    seqs, width = tokens.shape
    vmem = pl.BlockSpec(memory_space=pltpu.VMEM)
    bf16, f32 = jnp.bfloat16, jnp.float32
    part = pltpu.HBM((seqs, 512), bf16)
    hbm = pl.BlockSpec(memory_space=pltpu.HBM)
    either = pl.BlockSpec(memory_space=pl.ANY)
    return pl.pallas_call(
        expert_kernel,
        out_shape=(
            pltpu.HBM((1024, 128), bf16),
            pltpu.HBM((seqs, 512), f32),
            part,
            part,
            part,
        ),
        in_specs=[vmem] * 2 + [either] * 4 + [hbm] * 8,
        out_specs=(hbm,) * 5,
        scratch_shapes=[
            pltpu.VMEM((4, seqs, 256), bf16),
            pltpu.VMEM((seqs, 512), f32),
            pltpu.VMEM((3, seqs, 512), bf16),
            pltpu.VMEM((seqs, width), f32),
            pltpu.VMEM((seqs, width), bf16),
            pltpu.VMEM((1536, 128), f32),
            pltpu.VMEM((1024, 128), f32),
            pltpu.VMEM((1024, 128), bf16),
            pltpu.VMEM((seqs, width), bf16),
            pltpu.VMEM((1, width), f32),
            pltpu.VMEM(w_out.shape, bf16),
            pltpu.VMEM(w_up.shape[1:], bf16),
            pltpu.VMEM(w_down.shape[1:], bf16),
            pltpu.VMEM(w_shared_gate.shape, bf16),
            pltpu.VMEM(w_shared_up.shape, bf16),
            pltpu.VMEM(w_shared_down.shape, bf16),
            pltpu.SemaphoreType.DMA((11,)),
            pltpu.SemaphoreType.DMA((4,)),
            pltpu.SemaphoreType.DMA((6,)),
        ],
        compiler_params=pltpu.CompilerParams(vmem_limit_bytes=24 * 1024 * 1024),
        name="run_experts",
    )(
        rows,
        w_gate,
        *in_hbm(own_heads),
        *got_heads,
        *in_hbm(tokens, ffn_gain.reshape(1, -1), *weights),
    )


def finish_kernel(returned, combine, base, part_1, part_2, part_3, mixed, wide):
    seqs = base.shape[0]
    wide[...] = returned[...].astype(jnp.float32)
    arrived = jnp.concatenate(
        [
            jnp.concatenate(
                [
                    wide[pl.ds(2 * b + c, 128, stride=8), :].astype(jnp.bfloat16)
                    for b in range(4)
                ],
                axis=1,
            )
            for c in range(2)
        ],
        axis=0,
    )
    routed = jnp.dot(combine[...], arrived, preferred_element_type=jnp.float32)
    total = base[...]
    for part in (part_1, part_2, part_3):
        total = total + part[...].astype(jnp.float32)
    for k in range(3):
        total = total + routed[k * seqs : (k + 1) * seqs, :]
    mixed[...] = total.astype(jnp.bfloat16)


def finish(returned, combine, base, parts):
    vmem = pl.BlockSpec(memory_space=pltpu.VMEM)
    return pl.pallas_call(
        finish_kernel,
        out_shape=jax.ShapeDtypeStruct(base.shape, jnp.bfloat16),
        in_specs=[vmem] * 6,
        out_specs=vmem,
        scratch_shapes=[pltpu.VMEM((1024, 128), jnp.float32)],
        compiler_params=pltpu.CompilerParams(vmem_limit_bytes=4 * 1024 * 1024),
        name="finish",
    )(returned, combine, base, *parts)


def around(value, shift):
    count = lax.axis_size("tp")
    return lax.ppermute(value, "tp", [(i, (i + shift) % count) for i in range(count)])


def shards(
    tokens,
    kv_cache,
    lengths,
    attn_gain,
    w_query,
    w_key,
    w_value,
    lambdas,
    head_gain,
    w_out,
    ffn_gain,
    w_shared_gate,
    w_shared_up,
    w_shared_down,
    routing,
    route_weights,
    w_exp_gate,
    w_exp_up,
    w_exp_down,
):
    everyone = ("ep", "tp")
    message, heads, combine = attend(
        tokens,
        kv_cache,
        lengths,
        attn_gain,
        w_query,
        w_key,
        w_value,
        lambdas,
        head_gain,
        routing,
        route_weights,
    )
    message = message.reshape(128, 6, 2, 128)
    arrived = lax.all_to_all(message, everyone, split_axis=0, concat_axis=0, tiled=True)
    got_heads = [around(heads, k) for k in range(1, 4)]
    (gate,) = fetch(heads, (w_exp_gate,))
    rows = arrived.reshape(1536, 128)
    results, base, *parts = run_experts(
        rows,
        heads,
        got_heads,
        tokens,
        ffn_gain,
        gate,
        (w_out, w_exp_up, w_exp_down, w_shared_gate, w_shared_up, w_shared_down),
    )
    results = results.reshape(128, 4, 2, 128)
    returned = lax.all_to_all(results, everyone, split_axis=0, concat_axis=0, tiled=True)
    parts = [around(part, k + 1) for k, part in enumerate(parts)]
    combine, base = fetch(base, (combine, base))
    returned = returned.reshape(1024, 128)
    return finish(returned, combine, base, parts)


def solution(mesh):
    return jax.shard_map(
        shards,
        mesh=mesh,
        in_specs=(
            P("ep", None),
            P("ep", None, "tp"),
            P("ep"),
            P(),
            P(None, "tp"),
            P(None, "tp"),
            P(None, "tp"),
            P("tp"),
            P(),
            P(),
            P(),
            P(None, "tp"),
            P(None, "tp"),
            P("tp", None),
            P(),
            P("ep", None),
            P(("ep", "tp"), None, None),
            P(("ep", "tp"), None, None),
            P(("ep", "tp"), None, None),
        ),
        out_specs=P("ep", "tp"),
        check_vma=False,
    )
```

```python
import jax
import jax.numpy as jnp
from jax import lax
from jax.experimental import pallas as pl
from jax.experimental.pallas import tpu as pltpu
from jax.sharding import PartitionSpec as P

epsilon = 1e-06
neg_fill = -1e30
SPAN = 512
VMEM_BYTES = 64 * 1024 * 1024 - 65536


def attend_kernel(
    lengths_hbm,
    lambdas_hbm,
    tokens_hbm,
    gain_hbm,
    w_query_hbm,
    w_key_hbm,
    w_value_hbm,
    head_gain_hbm,
    routing_hbm,
    route_weights_hbm,
    kv_hbm,
    message,
    heads_out,
    combine_out,
    kv,
    lengths,
    lambdas,
    tokens,
    gain,
    w_query,
    w_key,
    w_value,
    head_gain,
    routing,
    route_weights,
    q8,
    n4,
    spread,
    scores,
    turned,
    values,
    mix,
    heads,
    combine,
    stage,
    ready,
    sems,
    kv_sems,
    send_sems,
):
    seqs, _ = tokens.shape
    cache_len = kv.shape[1]
    spans = cache_len // SPAN
    rows_all = seqs * 4

    def kv_copy(i):
        part = pl.ds(i * SPAN, SPAN)
        return pltpu.make_async_copy(kv_hbm.at[:, part], kv.at[:, part], kv_sems.at[i])

    loads = [
        pltpu.make_async_copy(src, dst, sems.at[i])
        for i, (src, dst) in enumerate(
            [
                (tokens_hbm, tokens),
                (gain_hbm, gain),
                (w_query_hbm, w_query),
                (w_key_hbm, w_key),
                (w_value_hbm, w_value),
                (routing_hbm, routing),
                (head_gain_hbm, head_gain),
                (route_weights_hbm, route_weights),
                (lengths_hbm, lengths),
                (lambdas_hbm, lambdas),
            ]
        )
    ]
    for load in loads:
        load.start()
    for i in range(spans):
        kv_copy(i).start()
    lane = lax.broadcasted_iota(jnp.int32, (1, 128), 1)
    loads[0].wait()
    loads[1].wait()
    wide = tokens[...].astype(jnp.float32)
    scale = lax.rsqrt(jnp.mean(wide * wide, axis=1, keepdims=True) + epsilon)
    normed = (wide * scale * gain[...]).astype(jnp.bfloat16)
    for load in loads[2:5]:
        load.wait()

    def rounded(value):
        return value.astype(jnp.bfloat16).astype(jnp.float32)

    def against(weight):
        return rounded(
            lax.dot_general(
                normed,
                weight[...],
                (((1,), (1,)), ((), ())),
                preferred_element_type=jnp.float32,
            )
        )

    queries = rounded(jnp.dot(normed, w_query[...], preferred_element_type=jnp.float32))
    new_row = jnp.concatenate([against(w_key), against(w_value)], axis=1)
    for head in range(4):
        pair = queries[:, 128 * (head // 2) : 128 * (head // 2) + 128]
        if head % 2:
            pair = pltpu.roll(pair, 64, 1)
        for half in range(2):
            own = (lane >= 32 * half) & (lane < 32 * half + 32)
            q8[pl.ds(half * rows_all + head, seqs, stride=4), :] = jnp.where(own, pair, 0.0)
        n4[pl.ds(head, seqs, stride=4), :] = new_row
    query_t = [q8[half * rows_all : (half + 1) * rows_all, :].T for half in range(2)]
    fresh = n4[...]
    fresh_t = fresh.T
    lane_seq = lax.broadcasted_iota(jnp.int32, (64, 128), 1) // 4
    for half in range(2):
        for s in range(seqs):
            spread[s * 64 : (s + 1) * 64, half * 128 : half * 128 + 128] = jnp.where(
                lane_seq == s, query_t[half][:64], 0.0
            ).astype(jnp.bfloat16)

    for load in loads[5:]:
        load.wait()
    place = (lax.axis_index("ep"), lax.axis_index("tp"))
    base = pl.multiple_of((place[0] // 4) * 128, 128)
    shift = 128 - (place[0] % 4) * 32
    named = jnp.where(lane < seqs, pltpu.roll(routing[:, pl.ds(base, 128)], shift, 1), -1)
    at_row = lax.broadcasted_iota(jnp.int32, (128, 128), 0)
    at_column = lax.broadcasted_iota(jnp.int32, (128, 128), 1)
    named_at = [at_row == named[k : k + 1, :] for k in range(4)]
    any_at = named_at[0] | named_at[1] | named_at[2] | named_at[3]
    before = (at_row < at_column).astype(jnp.float32).astype(jnp.bfloat16)
    rank = jnp.dot(
        any_at.astype(jnp.float32).astype(jnp.bfloat16),
        before,
        preferred_element_type=jnp.float32,
    )
    amount = jnp.zeros((128, 128), jnp.float32)
    widths = jnp.concatenate([route_weights[...]] * 4, axis=1)
    for k in range(4):
        amount = jnp.where(named_at[k], widths[k : k + 1, :], amount)
    picks = []
    for c in range(2):
        taken = any_at & (rank == float(c))
        picks.append(jnp.where(taken, 1.0, 0.0).astype(jnp.bfloat16)[:, :seqs])
        own_amount = jnp.where(taken, amount, 0.0).T[:seqs, :]
        for k in range(3):
            term = own_amount.astype(jnp.bfloat16)
            combine[k * seqs : (k + 1) * seqs, 128 * c : 128 * c + 128] = term
            own_amount = own_amount - term.astype(jnp.float32)

    def place_rows(source, first):
        for c in range(2):
            packed = jnp.dot(picks[c], source, preferred_element_type=jnp.float32)
            for b in range(source.shape[1] // 128):
                row = 2 * (first + b) + c
                stage[pl.ds(row, 128, stride=12), :] = packed[:, 128 * b : 128 * b + 128]

    share = tokens[:, pl.ds(pl.multiple_of(place[1] * 512, 128), 512)]
    place_rows(share, 2)

    scaling = 32 ** (-0.5)
    count = jnp.zeros((1, 128), jnp.int32)
    for s in range(seqs):
        count = jnp.where(lane // 4 == s, lengths[s], count)
    count = jnp.concatenate([count, count], axis=1)
    lam = jnp.zeros((1, 128), jnp.float32)
    for head in range(4):
        lam = jnp.where(lane % 4 == head, lambdas[head], lam)
    score_new = [
        jnp.sum(query_t[half] * fresh_t, axis=0, keepdims=True) * scaling for half in range(2)
    ]
    score_new = jnp.concatenate(score_new, axis=1)

    position = lax.broadcasted_iota(jnp.int32, (SPAN, 256), 0)
    highest = score_new
    for i in range(spans):
        kv_copy(i).wait()
        cut = slice(i * SPAN, (i + 1) * SPAN)
        keys = []
        for pair in range(seqs // 2):
            one = kv[2 * pair, cut, :]
            two = pltpu.roll(kv[2 * pair + 1, cut, :], 64, 1)
            keys.append(jnp.where(lane < 64, one, two))
            values[pair, cut, :] = jnp.where(lane < 64, two, one)
        part = jnp.concatenate(keys, axis=1)
        found = jnp.dot(part, spread[...], preferred_element_type=jnp.float32) * scaling
        found = jnp.where(position < count - i * SPAN, found, neg_fill)
        scores[i * SPAN : (i + 1) * SPAN, :] = found
        highest = jnp.maximum(highest, jnp.max(found, axis=0, keepdims=True))
    expo_new = jnp.exp(score_new - highest)
    total = expo_new
    for i in range(spans):
        found = scores[i * SPAN : (i + 1) * SPAN, :]
        expo = jnp.where(position < count - i * SPAN, jnp.exp(found - highest), 0.0)
        scores[i * SPAN : (i + 1) * SPAN, :] = expo
        total = total + jnp.sum(expo, axis=0, keepdims=True)
    factor = 1.0 / total
    first = factor[:, :128]
    second = lam * factor[:, 128:]
    for i in range(cache_len // 128):
        expo = scores[i * 128 : (i + 1) * 128, :]
        weight = expo[:, :128] * first - expo[:, 128:] * second
        turned[:, i * 128 : (i + 1) * 128] = weight.T.astype(jnp.bfloat16)
    weight_new = expo_new[:, :128] * first - expo_new[:, 128:] * second
    diagonal = jnp.where(at_row == at_column, weight_new, 0.0).astype(jnp.bfloat16)
    mix_new = jnp.dot(diagonal, fresh.astype(jnp.bfloat16), preferred_element_type=jnp.float32)
    row16 = lax.broadcasted_iota(jnp.int32, (16, 1), 0)
    for i in range(seqs // 4):
        four = jnp.concatenate([values[2 * i], values[2 * i + 1]], axis=1)
        out = jnp.dot(turned[16 * i : 16 * i + 16, :], four, preferred_element_type=jnp.float32)
        left, right = out[:, :128], out[:, 128:]
        upper = jnp.where(row16 < 4, left, pltpu.roll(left, 64, 1))
        lower = jnp.where(row16 < 12, right, pltpu.roll(right, 64, 1))
        mix[16 * i : 16 * i + 16, :] = jnp.where(row16 < 8, upper, lower)

    blend = mix[...] + mix_new
    own = jnp.where(lane >= 64, blend, 0.0)
    power = jnp.sum(own * own, axis=1, keepdims=True) * (1.0 / 64)
    gain2 = jnp.concatenate([head_gain[...], head_gain[...]], axis=1)
    mix[...] = blend * lax.rsqrt(power + epsilon) * gain2
    pieces = []
    for pair in range(2):
        even = mix[pl.ds(2 * pair, seqs, stride=4), :]
        odd = mix[pl.ds(2 * pair + 1, seqs, stride=4), :]
        both = jnp.where(lane < 64, pltpu.roll(even, 64, 1), odd).astype(jnp.bfloat16)
        heads[:, 128 * pair : 128 * pair + 128] = both
        pieces.append(both)
    extra = [
        pltpu.make_async_copy(heads, heads_out, send_sems.at[4]),
        pltpu.make_async_copy(combine, combine_out, send_sems.at[5]),
    ]
    for send in extra:
        send.start()
    place_rows(jnp.concatenate(pieces, axis=1), 0)
    sends = []
    for i in range(4):
        part = pl.ds(384 * i, 384)
        ready[part, :] = stage[part, :].astype(jnp.bfloat16)
        sends.append(
            pltpu.make_async_copy(ready.at[part], message.at[part], send_sems.at[i])
        )
        sends[i].start()
    for send in sends + extra:
        send.wait()


def in_hbm(*arrays):
    return [pltpu.with_memory_space_constraint(array, pltpu.HBM) for array in arrays]


def attend(
    tokens, kv_cache, lengths, gain, w_query, w_key, w_value, lambdas, head_gain, routing,
    route_weights,
):
    seqs, width = tokens.shape
    hbm = pl.BlockSpec(memory_space=pltpu.HBM)
    bf16, f32 = jnp.bfloat16, jnp.float32
    return pl.pallas_call(
        attend_kernel,
        out_shape=(
            pltpu.HBM((1536, 128), bf16),
            pltpu.HBM((seqs, 256), bf16),
            pltpu.HBM((3 * seqs, 256), bf16),
        ),
        in_specs=[hbm] * 11,
        out_specs=(hbm, hbm, hbm),
        scratch_shapes=[
            pltpu.VMEM(kv_cache.shape, bf16),
            pltpu.SMEM((seqs,), jnp.int32),
            pltpu.SMEM((4,), f32),
            pltpu.VMEM((seqs, width), bf16),
            pltpu.VMEM((1, width), f32),
            pltpu.VMEM((width, 256), bf16),
            pltpu.VMEM((64, width), bf16),
            pltpu.VMEM((64, width), bf16),
            pltpu.VMEM((1, 64), f32),
            pltpu.VMEM((4, routing.shape[0]), jnp.int32),
            pltpu.VMEM((4, seqs), f32),
            pltpu.VMEM((seqs * 8, 128), f32),
            pltpu.VMEM((seqs * 4, 128), f32),
            pltpu.VMEM((seqs * 64, 256), bf16),
            pltpu.VMEM((kv_cache.shape[1], 256), f32),
            pltpu.VMEM((128, kv_cache.shape[1]), bf16),
            pltpu.VMEM((seqs // 2, kv_cache.shape[1], 128), bf16),
            pltpu.VMEM((seqs * 4, 128), f32),
            pltpu.VMEM((seqs, 256), bf16),
            pltpu.VMEM((3 * seqs, 256), bf16),
            pltpu.VMEM((1536, 128), f32),
            pltpu.VMEM((1536, 128), bf16),
            pltpu.SemaphoreType.DMA((10,)),
            pltpu.SemaphoreType.DMA((kv_cache.shape[1] // SPAN,)),
            pltpu.SemaphoreType.DMA((6,)),
        ],
        compiler_params=pltpu.CompilerParams(vmem_limit_bytes=VMEM_BYTES),
        name="attend",
    )(
        *in_hbm(
            lengths,
            lambdas,
            tokens,
            gain.reshape(1, -1),
            w_query,
            w_key.T,
            w_value.T,
            head_gain.reshape(1, -1),
            routing.T,
            route_weights.T,
            kv_cache,
        )
    )


def fetch_kernel(after, *refs):
    count = (len(refs) - 1) // 2
    loads = [
        pltpu.make_async_copy(refs[i], refs[count + i], refs[-1].at[i]) for i in range(count)
    ]
    for load in loads:
        load.start()
    for load in loads:
        load.wait()


def fetch(after, arrays):
    hbm = pl.BlockSpec(memory_space=pltpu.HBM)
    return pl.pallas_call(
        fetch_kernel,
        out_shape=tuple(jax.ShapeDtypeStruct(a.shape, a.dtype) for a in arrays),
        in_specs=[hbm] * (1 + len(arrays)),
        out_specs=(pl.BlockSpec(memory_space=pltpu.VMEM),) * len(arrays),
        scratch_shapes=[pltpu.SemaphoreType.DMA((len(arrays),))],
        compiler_params=pltpu.CompilerParams(vmem_limit_bytes=1024 * 1024),
        name="fetch",
    )(*in_hbm(after, *arrays))


def expert_kernel(
    rows,
    w_gate,
    w_shared_gate,
    own_heads,
    heads_1,
    heads_2,
    heads_3,
    tokens_hbm,
    ffn_gain_hbm,
    w_out_hbm,
    w_up_hbm,
    w_down_hbm,
    w_shared_up_hbm,
    w_shared_down_hbm,
    results,
    base_out,
    part_1,
    part_2,
    part_3,
    heads,
    base,
    parts,
    partial,
    resid,
    wide_rows,
    stage,
    ready,
    tokens,
    ffn_gain,
    w_out,
    w_up,
    w_down,
    w_shared_up,
    w_shared_down,
    sems,
    head_sems,
    send_sems,
):
    slots = 64
    quarters = [pl.ds(256 * t, 256) for t in range(4)]
    gathered = [
        pltpu.make_async_copy(got, heads.at[k], head_sems.at[k])
        for k, got in enumerate((own_heads, heads_1, heads_2, heads_3))
    ]
    for load in gathered:
        load.start()
    loads = [(w_out_hbm.at[quarter], w_out.at[quarter]) for quarter in quarters]
    loads += [(tokens_hbm, tokens), (ffn_gain_hbm, ffn_gain)]
    loads += [(w_up_hbm.at[0], w_up), (w_down_hbm.at[0], w_down)]
    loads += [(w_shared_up_hbm, w_shared_up), (w_shared_down_hbm, w_shared_down)]
    loads = [
        pltpu.make_async_copy(source, target, sems.at[i])
        for i, (source, target) in enumerate(loads)
    ]
    for load in loads:
        load.start()
    wide_rows[...] = rows[...].astype(jnp.float32)

    def arrived_rows(t, b):
        halves = [
            wide_rows[pl.ds(12 * t + 2 * b + c, 32, stride=48), :].astype(jnp.bfloat16)
            for c in range(2)
        ]
        return jnp.concatenate(halves, axis=0)

    for load in gathered:
        load.wait()
    tp = lax.axis_index("tp")
    total = None
    for t in range(4):
        arrived = jnp.concatenate([arrived_rows(t, 0), arrived_rows(t, 1)], axis=1)
        both = jnp.concatenate([arrived, heads[(tp + 4 - t) % 4]], axis=0)
        loads[t].wait()
        piece = jnp.dot(
            both, w_out[256 * t : 256 * t + 256, :], preferred_element_type=jnp.float32
        )
        piece = piece.astype(jnp.bfloat16).astype(jnp.float32)
        total = piece if total is None else total + piece
    row_tokens = jnp.concatenate([arrived_rows(t, b) for t in range(4) for b in range(2, 6)], axis=1)
    loads[4].wait()
    loads[5].wait()
    all_tokens = jnp.concatenate([row_tokens, tokens[...]], axis=0)
    residual = (all_tokens.astype(jnp.float32) + total).astype(jnp.bfloat16)
    resid[...] = residual[slots:]
    wide = residual.astype(jnp.float32)
    scale = lax.rsqrt(jnp.mean(wide * wide, axis=1, keepdims=True) + epsilon)
    ffn_in = (wide * scale * ffn_gain[...]).astype(jnp.bfloat16)

    def gated(value, gate, up):
        gate_part = jnp.dot(value, gate, preferred_element_type=jnp.float32)
        up_part = jnp.dot(value, up, preferred_element_type=jnp.float32)
        return (gate_part / (1.0 + jnp.exp(-gate_part)) * up_part).astype(jnp.bfloat16)

    loads[6].wait()
    act = gated(ffn_in[:slots], w_gate[0], w_up[...])
    loads[7].wait()
    result = jnp.dot(act, w_down[...], preferred_element_type=jnp.float32)
    for b in range(16):
        for c in range(2):
            stage[pl.ds(2 * b + c, 32, stride=32), :] = result[
                32 * c : 32 * c + 32, 128 * b : 128 * b + 128
            ]
    sends = []
    for i in range(2):
        half = pl.ds(512 * i, 512)
        ready[half, :] = stage[half, :].astype(jnp.bfloat16)
        sends.append(pltpu.make_async_copy(ready.at[half], results.at[half], send_sems.at[i]))
        sends[i].start()
    loads[8].wait()
    shared_act = gated(ffn_in[slots:], w_shared_gate[...], w_shared_up[...])
    loads[9].wait()
    partial[...] = jnp.dot(shared_act, w_shared_down[...], preferred_element_type=jnp.float32)

    def share(source, shift):
        at = pl.multiple_of(((tp + shift) % 4) * 512, 512)
        return source[:, pl.ds(at, 512)]

    for k, part in enumerate((part_1, part_2, part_3)):
        parts[k] = share(partial, k + 1).astype(jnp.bfloat16)
        sends.append(pltpu.make_async_copy(parts.at[k], part, send_sems.at[2 + k]))
        sends[2 + k].start()
    base[...] = share(partial, 0) + share(resid, 0).astype(jnp.float32)
    sends.append(pltpu.make_async_copy(base, base_out, send_sems.at[5]))
    sends[5].start()
    for send in sends:
        send.wait()


def run_experts(rows, own_heads, got_heads, tokens, ffn_gain, early, weights):
    w_out, w_up, w_down, w_shared_up, w_shared_down = weights
    seqs, width = tokens.shape
    vmem = pl.BlockSpec(memory_space=pltpu.VMEM)
    bf16, f32 = jnp.bfloat16, jnp.float32
    part = pltpu.HBM((seqs, 512), bf16)
    hbm = pl.BlockSpec(memory_space=pltpu.HBM)
    either = pl.BlockSpec(memory_space=pl.ANY)
    return pl.pallas_call(
        expert_kernel,
        out_shape=(
            pltpu.HBM((1024, 128), bf16),
            pltpu.HBM((seqs, 512), f32),
            part,
            part,
            part,
        ),
        in_specs=[vmem] * 3 + [either] * 4 + [hbm] * 7,
        out_specs=(hbm,) * 5,
        scratch_shapes=[
            pltpu.VMEM((4, seqs, 256), bf16),
            pltpu.VMEM((seqs, 512), f32),
            pltpu.VMEM((3, seqs, 512), bf16),
            pltpu.VMEM((seqs, width), f32),
            pltpu.VMEM((seqs, width), bf16),
            pltpu.VMEM((1536, 128), f32),
            pltpu.VMEM((1024, 128), f32),
            pltpu.VMEM((1024, 128), bf16),
            pltpu.VMEM((seqs, width), bf16),
            pltpu.VMEM((1, width), f32),
            pltpu.VMEM(w_out.shape, bf16),
            pltpu.VMEM(w_up.shape[1:], bf16),
            pltpu.VMEM(w_down.shape[1:], bf16),
            pltpu.VMEM(w_shared_up.shape, bf16),
            pltpu.VMEM(w_shared_down.shape, bf16),
            pltpu.SemaphoreType.DMA((10,)),
            pltpu.SemaphoreType.DMA((4,)),
            pltpu.SemaphoreType.DMA((6,)),
        ],
        compiler_params=pltpu.CompilerParams(vmem_limit_bytes=24 * 1024 * 1024),
        name="run_experts",
    )(
        rows,
        *early,
        *in_hbm(own_heads),
        *got_heads,
        *in_hbm(tokens, ffn_gain.reshape(1, -1), *weights),
    )


def finish_kernel(returned, combine, base, part_1, part_2, part_3, mixed, wide):
    seqs = base.shape[0]
    wide[...] = returned[...].astype(jnp.float32)
    arrived = jnp.concatenate(
        [
            jnp.concatenate(
                [
                    wide[pl.ds(2 * b + c, 128, stride=8), :].astype(jnp.bfloat16)
                    for b in range(4)
                ],
                axis=1,
            )
            for c in range(2)
        ],
        axis=0,
    )
    routed = jnp.dot(combine[...], arrived, preferred_element_type=jnp.float32)
    total = base[...]
    for part in (part_1, part_2, part_3):
        total = total + part[...].astype(jnp.float32)
    for k in range(3):
        total = total + routed[k * seqs : (k + 1) * seqs, :]
    mixed[...] = total.astype(jnp.bfloat16)


def finish(returned, combine, base, parts):
    vmem = pl.BlockSpec(memory_space=pltpu.VMEM)
    return pl.pallas_call(
        finish_kernel,
        out_shape=jax.ShapeDtypeStruct(base.shape, jnp.bfloat16),
        in_specs=[vmem] * 6,
        out_specs=vmem,
        scratch_shapes=[pltpu.VMEM((1024, 128), jnp.float32)],
        compiler_params=pltpu.CompilerParams(vmem_limit_bytes=4 * 1024 * 1024),
        name="finish",
    )(returned, combine, base, *parts)


def around(value, shift):
    count = lax.axis_size("tp")
    return lax.ppermute(value, "tp", [(i, (i + shift) % count) for i in range(count)])


def shards(
    tokens,
    kv_cache,
    lengths,
    attn_gain,
    w_query,
    w_key,
    w_value,
    lambdas,
    head_gain,
    w_out,
    ffn_gain,
    w_shared_gate,
    w_shared_up,
    w_shared_down,
    routing,
    route_weights,
    w_exp_gate,
    w_exp_up,
    w_exp_down,
):
    everyone = ("ep", "tp")
    message, heads, combine = attend(
        tokens,
        kv_cache,
        lengths,
        attn_gain,
        w_query,
        w_key,
        w_value,
        lambdas,
        head_gain,
        routing,
        route_weights,
    )
    message = message.reshape(128, 6, 2, 128)
    arrived = lax.all_to_all(message, everyone, split_axis=0, concat_axis=0, tiled=True)
    got_heads = [around(heads, k) for k in range(1, 4)]
    early = fetch(heads, (w_exp_gate, w_shared_gate))
    rows = arrived.reshape(1536, 128)
    results, base, *parts = run_experts(
        rows,
        heads,
        got_heads,
        tokens,
        ffn_gain,
        early,
        (w_out, w_exp_up, w_exp_down, w_shared_up, w_shared_down),
    )
    results = results.reshape(128, 4, 2, 128)
    returned = lax.all_to_all(results, everyone, split_axis=0, concat_axis=0, tiled=True)
    parts = [around(part, k + 1) for k, part in enumerate(parts)]
    combine, base = fetch(base, (combine, base))
    returned = returned.reshape(1024, 128)
    return finish(returned, combine, base, parts)


def solution(mesh):
    return jax.shard_map(
        shards,
        mesh=mesh,
        in_specs=(
            P("ep", None),
            P("ep", None, "tp"),
            P("ep"),
            P(),
            P(None, "tp"),
            P(None, "tp"),
            P(None, "tp"),
            P("tp"),
            P(),
            P(),
            P(),
            P(None, "tp"),
            P(None, "tp"),
            P("tp", None),
            P(),
            P("ep", None),
            P(("ep", "tp"), None, None),
            P(("ep", "tp"), None, None),
            P(("ep", "tp"), None, None),
        ),
        out_specs=P("ep", "tp"),
        check_vma=False,
    )
```

```python
import jax
import jax.numpy as jnp
from jax import lax
from jax.experimental import pallas as pl
from jax.experimental.pallas import tpu as pltpu
from jax.sharding import PartitionSpec as P

epsilon = 1e-06
neg_fill = -1e30
SPAN = 512
VMEM_BYTES = 64 * 1024 * 1024 - 65536


def attend_kernel(
    lengths_hbm,
    lambdas_hbm,
    tokens_hbm,
    gain_hbm,
    w_query_hbm,
    w_key_hbm,
    w_value_hbm,
    head_gain_hbm,
    routing_hbm,
    route_weights_hbm,
    kv_hbm,
    message,
    heads_out,
    combine_out,
    kv,
    lengths,
    lambdas,
    tokens,
    gain,
    w_query,
    w_key,
    w_value,
    head_gain,
    routing,
    route_weights,
    q8,
    n4,
    spread,
    scores,
    turned,
    values,
    mix,
    heads,
    combine,
    stage,
    ready,
    sems,
    kv_sems,
    send_sems,
):
    seqs, _ = tokens.shape
    cache_len = kv.shape[1]
    spans = cache_len // SPAN
    rows_all = seqs * 4

    def kv_copy(i):
        part = pl.ds(i * SPAN, SPAN)
        return pltpu.make_async_copy(kv_hbm.at[:, part], kv.at[:, part], kv_sems.at[i])

    loads = [
        pltpu.make_async_copy(src, dst, sems.at[i])
        for i, (src, dst) in enumerate(
            [
                (tokens_hbm, tokens),
                (gain_hbm, gain),
                (w_query_hbm, w_query),
                (w_key_hbm, w_key),
                (w_value_hbm, w_value),
                (routing_hbm, routing),
                (head_gain_hbm, head_gain),
                (route_weights_hbm, route_weights),
                (lengths_hbm, lengths),
                (lambdas_hbm, lambdas),
            ]
        )
    ]
    for load in loads:
        load.start()
    for i in range(spans):
        kv_copy(i).start()
    lane = lax.broadcasted_iota(jnp.int32, (1, 128), 1)
    loads[0].wait()
    loads[1].wait()
    wide = tokens[...].astype(jnp.float32)
    scale = lax.rsqrt(jnp.mean(wide * wide, axis=1, keepdims=True) + epsilon)
    normed = (wide * scale * gain[...]).astype(jnp.bfloat16)
    for load in loads[2:5]:
        load.wait()

    def rounded(value):
        return value.astype(jnp.bfloat16).astype(jnp.float32)

    def against(weight):
        return rounded(
            lax.dot_general(
                normed,
                weight[...],
                (((1,), (1,)), ((), ())),
                preferred_element_type=jnp.float32,
            )
        )

    queries = rounded(jnp.dot(normed, w_query[...], preferred_element_type=jnp.float32))
    new_row = jnp.concatenate([against(w_key), against(w_value)], axis=1)
    for head in range(4):
        pair = queries[:, 128 * (head // 2) : 128 * (head // 2) + 128]
        if head % 2:
            pair = pltpu.roll(pair, 64, 1)
        for half in range(2):
            own = (lane >= 32 * half) & (lane < 32 * half + 32)
            q8[pl.ds(half * rows_all + head, seqs, stride=4), :] = jnp.where(own, pair, 0.0)
        n4[pl.ds(head, seqs, stride=4), :] = new_row
    query_t = [q8[half * rows_all : (half + 1) * rows_all, :].T for half in range(2)]
    fresh = n4[...]
    fresh_t = fresh.T
    lane_seq = lax.broadcasted_iota(jnp.int32, (64, 128), 1) // 4
    for half in range(2):
        for s in range(seqs):
            spread[s * 64 : (s + 1) * 64, half * 128 : half * 128 + 128] = jnp.where(
                lane_seq == s, query_t[half][:64], 0.0
            ).astype(jnp.bfloat16)

    for load in loads[5:]:
        load.wait()
    place = (lax.axis_index("ep"), lax.axis_index("tp"))
    base = pl.multiple_of((place[0] // 4) * 128, 128)
    shift = 128 - (place[0] % 4) * 32
    named = jnp.where(lane < seqs, pltpu.roll(routing[:, pl.ds(base, 128)], shift, 1), -1)
    at_row = lax.broadcasted_iota(jnp.int32, (128, 128), 0)
    at_column = lax.broadcasted_iota(jnp.int32, (128, 128), 1)
    named_at = [at_row == named[k : k + 1, :] for k in range(4)]
    any_at = named_at[0] | named_at[1] | named_at[2] | named_at[3]
    before = (at_row < at_column).astype(jnp.float32).astype(jnp.bfloat16)
    rank = jnp.dot(
        any_at.astype(jnp.float32).astype(jnp.bfloat16),
        before,
        preferred_element_type=jnp.float32,
    )
    amount = jnp.zeros((128, 128), jnp.float32)
    widths = jnp.concatenate([route_weights[...]] * 4, axis=1)
    for k in range(4):
        amount = jnp.where(named_at[k], widths[k : k + 1, :], amount)
    picks = []
    for c in range(2):
        taken = any_at & (rank == float(c))
        picks.append(jnp.where(taken, 1.0, 0.0).astype(jnp.bfloat16)[:, :seqs])
        own_amount = jnp.where(taken, amount, 0.0).T[:seqs, :]
        for k in range(3):
            term = own_amount.astype(jnp.bfloat16)
            combine[k * seqs : (k + 1) * seqs, 128 * c : 128 * c + 128] = term
            own_amount = own_amount - term.astype(jnp.float32)

    def place_rows(source, first):
        for c in range(2):
            packed = jnp.dot(picks[c], source, preferred_element_type=jnp.float32)
            for b in range(source.shape[1] // 128):
                row = 2 * (first + b) + c
                stage[pl.ds(row, 128, stride=12), :] = packed[:, 128 * b : 128 * b + 128]

    share = tokens[:, pl.ds(pl.multiple_of(place[1] * 512, 128), 512)]
    place_rows(share, 2)

    scaling = 32 ** (-0.5)
    count = jnp.zeros((1, 128), jnp.int32)
    for s in range(seqs):
        count = jnp.where(lane // 4 == s, lengths[s], count)
    count = jnp.concatenate([count, count], axis=1)
    lam = jnp.zeros((1, 128), jnp.float32)
    for head in range(4):
        lam = jnp.where(lane % 4 == head, lambdas[head], lam)
    score_new = [
        jnp.sum(query_t[half] * fresh_t, axis=0, keepdims=True) * scaling for half in range(2)
    ]
    score_new = jnp.concatenate(score_new, axis=1)

    position = lax.broadcasted_iota(jnp.int32, (SPAN, 256), 0)
    highest = score_new
    for i in range(spans):
        kv_copy(i).wait()
        cut = slice(i * SPAN, (i + 1) * SPAN)
        keys = []
        for pair in range(seqs // 2):
            one = kv[2 * pair, cut, :]
            two = pltpu.roll(kv[2 * pair + 1, cut, :], 64, 1)
            keys.append(jnp.where(lane < 64, one, two))
            values[pair, cut, :] = jnp.where(lane < 64, two, one)
        part = jnp.concatenate(keys, axis=1)
        found = jnp.dot(part, spread[...], preferred_element_type=jnp.float32) * scaling
        found = jnp.where(position < count - i * SPAN, found, neg_fill)
        scores[i * SPAN : (i + 1) * SPAN, :] = found
        highest = jnp.maximum(highest, jnp.max(found, axis=0, keepdims=True))
    expo_new = jnp.exp(score_new - highest)
    total = expo_new
    for i in range(spans):
        found = scores[i * SPAN : (i + 1) * SPAN, :]
        expo = jnp.where(position < count - i * SPAN, jnp.exp(found - highest), 0.0)
        scores[i * SPAN : (i + 1) * SPAN, :] = expo
        total = total + jnp.sum(expo, axis=0, keepdims=True)
    factor = 1.0 / total
    first = factor[:, :128]
    second = lam * factor[:, 128:]
    for i in range(cache_len // 128):
        expo = scores[i * 128 : (i + 1) * 128, :]
        weight = expo[:, :128] * first - expo[:, 128:] * second
        turned[:, i * 128 : (i + 1) * 128] = weight.T.astype(jnp.bfloat16)
    weight_new = expo_new[:, :128] * first - expo_new[:, 128:] * second
    diagonal = jnp.where(at_row == at_column, weight_new, 0.0).astype(jnp.bfloat16)
    mix_new = jnp.dot(diagonal, fresh.astype(jnp.bfloat16), preferred_element_type=jnp.float32)
    row16 = lax.broadcasted_iota(jnp.int32, (16, 1), 0)
    for i in range(seqs // 4):
        four = jnp.concatenate([values[2 * i], values[2 * i + 1]], axis=1)
        out = jnp.dot(turned[16 * i : 16 * i + 16, :], four, preferred_element_type=jnp.float32)
        left, right = out[:, :128], out[:, 128:]
        upper = jnp.where(row16 < 4, left, pltpu.roll(left, 64, 1))
        lower = jnp.where(row16 < 12, right, pltpu.roll(right, 64, 1))
        mix[16 * i : 16 * i + 16, :] = jnp.where(row16 < 8, upper, lower)

    blend = mix[...] + mix_new
    own = jnp.where(lane >= 64, blend, 0.0)
    power = jnp.sum(own * own, axis=1, keepdims=True) * (1.0 / 64)
    gain2 = jnp.concatenate([head_gain[...], head_gain[...]], axis=1)
    mix[...] = blend * lax.rsqrt(power + epsilon) * gain2
    pieces = []
    for pair in range(2):
        even = mix[pl.ds(2 * pair, seqs, stride=4), :]
        odd = mix[pl.ds(2 * pair + 1, seqs, stride=4), :]
        both = jnp.where(lane < 64, pltpu.roll(even, 64, 1), odd).astype(jnp.bfloat16)
        heads[:, 128 * pair : 128 * pair + 128] = both
        pieces.append(both)
    extra = [
        pltpu.make_async_copy(heads, heads_out, send_sems.at[4]),
        pltpu.make_async_copy(combine, combine_out, send_sems.at[5]),
    ]
    for send in extra:
        send.start()
    place_rows(jnp.concatenate(pieces, axis=1), 0)
    sends = []
    for i in range(4):
        part = pl.ds(384 * i, 384)
        ready[part, :] = stage[part, :].astype(jnp.bfloat16)
        sends.append(
            pltpu.make_async_copy(ready.at[part], message.at[part], send_sems.at[i])
        )
        sends[i].start()
    for send in sends + extra:
        send.wait()


def in_hbm(*arrays):
    return [pltpu.with_memory_space_constraint(array, pltpu.HBM) for array in arrays]


def attend(
    tokens, kv_cache, lengths, gain, w_query, w_key, w_value, lambdas, head_gain, routing,
    route_weights,
):
    seqs, width = tokens.shape
    hbm = pl.BlockSpec(memory_space=pltpu.HBM)
    bf16, f32 = jnp.bfloat16, jnp.float32
    return pl.pallas_call(
        attend_kernel,
        out_shape=(
            pltpu.HBM((1536, 128), bf16),
            pltpu.HBM((seqs, 256), bf16),
            pltpu.HBM((3 * seqs, 256), bf16),
        ),
        in_specs=[hbm] * 11,
        out_specs=(hbm, hbm, hbm),
        scratch_shapes=[
            pltpu.VMEM(kv_cache.shape, bf16),
            pltpu.SMEM((seqs,), jnp.int32),
            pltpu.SMEM((4,), f32),
            pltpu.VMEM((seqs, width), bf16),
            pltpu.VMEM((1, width), f32),
            pltpu.VMEM((width, 256), bf16),
            pltpu.VMEM((64, width), bf16),
            pltpu.VMEM((64, width), bf16),
            pltpu.VMEM((1, 64), f32),
            pltpu.VMEM((4, routing.shape[0]), jnp.int32),
            pltpu.VMEM((4, seqs), f32),
            pltpu.VMEM((seqs * 8, 128), f32),
            pltpu.VMEM((seqs * 4, 128), f32),
            pltpu.VMEM((seqs * 64, 256), bf16),
            pltpu.VMEM((kv_cache.shape[1], 256), f32),
            pltpu.VMEM((128, kv_cache.shape[1]), bf16),
            pltpu.VMEM((seqs // 2, kv_cache.shape[1], 128), bf16),
            pltpu.VMEM((seqs * 4, 128), f32),
            pltpu.VMEM((seqs, 256), bf16),
            pltpu.VMEM((3 * seqs, 256), bf16),
            pltpu.VMEM((1536, 128), f32),
            pltpu.VMEM((1536, 128), bf16),
            pltpu.SemaphoreType.DMA((10,)),
            pltpu.SemaphoreType.DMA((kv_cache.shape[1] // SPAN,)),
            pltpu.SemaphoreType.DMA((6,)),
        ],
        compiler_params=pltpu.CompilerParams(vmem_limit_bytes=VMEM_BYTES),
        name="attend",
    )(
        *in_hbm(
            lengths,
            lambdas,
            tokens,
            gain.reshape(1, -1),
            w_query,
            w_key.T,
            w_value.T,
            head_gain.reshape(1, -1),
            routing.T,
            route_weights.T,
            kv_cache,
        )
    )


def fetch_kernel(after, *refs):
    count = (len(refs) - 1) // 2
    loads = [
        pltpu.make_async_copy(refs[i], refs[count + i], refs[-1].at[i]) for i in range(count)
    ]
    for load in loads:
        load.start()
    for load in loads:
        load.wait()


def fetch(after, arrays):
    hbm = pl.BlockSpec(memory_space=pltpu.HBM)
    return pl.pallas_call(
        fetch_kernel,
        out_shape=tuple(jax.ShapeDtypeStruct(a.shape, a.dtype) for a in arrays),
        in_specs=[hbm] * (1 + len(arrays)),
        out_specs=(pl.BlockSpec(memory_space=pltpu.VMEM),) * len(arrays),
        scratch_shapes=[pltpu.SemaphoreType.DMA((len(arrays),))],
        compiler_params=pltpu.CompilerParams(vmem_limit_bytes=1024 * 1024),
        name="fetch",
    )(*in_hbm(after, *arrays))


def expert_kernel(
    rows,
    w_gate,
    own_heads,
    heads_1,
    heads_2,
    heads_3,
    tokens_hbm,
    ffn_gain_hbm,
    w_out_hbm,
    w_up_hbm,
    w_down_hbm,
    w_shared_gate_hbm,
    w_shared_up_hbm,
    w_shared_down_hbm,
    results,
    base_out,
    part_1,
    part_2,
    part_3,
    heads,
    base,
    parts,
    partial,
    resid,
    wide_rows,
    stage,
    ready,
    tokens,
    ffn_gain,
    w_out,
    w_up,
    w_down,
    w_shared_gate,
    w_shared_up,
    w_shared_down,
    sems,
    head_sems,
    send_sems,
):
    slots = 64
    quarters = [pl.ds(256 * t, 256) for t in range(4)]
    gathered = [
        pltpu.make_async_copy(got, heads.at[k], head_sems.at[k])
        for k, got in enumerate((own_heads, heads_1, heads_2, heads_3))
    ]
    for load in gathered:
        load.start()
    loads = [(w_out_hbm.at[quarter], w_out.at[quarter]) for quarter in quarters]
    loads += [(tokens_hbm, tokens), (ffn_gain_hbm, ffn_gain)]
    loads += [(w_shared_gate_hbm, w_shared_gate), (w_shared_up_hbm, w_shared_up)]
    loads += [(w_up_hbm.at[0], w_up), (w_down_hbm.at[0], w_down)]
    loads += [(w_shared_down_hbm, w_shared_down)]
    loads = [
        pltpu.make_async_copy(source, target, sems.at[i])
        for i, (source, target) in enumerate(loads)
    ]
    for load in loads:
        load.start()
    wide_rows[...] = rows[...].astype(jnp.float32)

    def arrived_rows(t, b):
        halves = [
            wide_rows[pl.ds(12 * t + 2 * b + c, 32, stride=48), :].astype(jnp.bfloat16)
            for c in range(2)
        ]
        return jnp.concatenate(halves, axis=0)

    for load in gathered:
        load.wait()
    tp = lax.axis_index("tp")
    total = None
    for t in range(4):
        arrived = jnp.concatenate([arrived_rows(t, 0), arrived_rows(t, 1)], axis=1)
        both = jnp.concatenate([arrived, heads[(tp + 4 - t) % 4]], axis=0)
        loads[t].wait()
        piece = jnp.dot(
            both, w_out[256 * t : 256 * t + 256, :], preferred_element_type=jnp.float32
        )
        piece = piece.astype(jnp.bfloat16).astype(jnp.float32)
        total = piece if total is None else total + piece
    row_tokens = jnp.concatenate([arrived_rows(t, b) for t in range(4) for b in range(2, 6)], axis=1)
    loads[4].wait()
    loads[5].wait()
    all_tokens = jnp.concatenate([row_tokens, tokens[...]], axis=0)
    residual = (all_tokens.astype(jnp.float32) + total).astype(jnp.bfloat16)
    resid[...] = residual[slots:]
    wide = residual.astype(jnp.float32)
    scale = lax.rsqrt(jnp.mean(wide * wide, axis=1, keepdims=True) + epsilon)
    ffn_in = (wide * scale * ffn_gain[...]).astype(jnp.bfloat16)

    def gated(value, gate, up):
        gate_part = jnp.dot(value, gate, preferred_element_type=jnp.float32)
        up_part = jnp.dot(value, up, preferred_element_type=jnp.float32)
        return (gate_part / (1.0 + jnp.exp(-gate_part)) * up_part).astype(jnp.bfloat16)

    loads[6].wait()
    loads[7].wait()
    shared_act = gated(ffn_in[slots:], w_shared_gate[...], w_shared_up[...])
    loads[8].wait()
    act = gated(ffn_in[:slots], w_gate[0], w_up[...])
    loads[9].wait()
    result = jnp.dot(act, w_down[...], preferred_element_type=jnp.float32)
    for b in range(16):
        for c in range(2):
            stage[pl.ds(2 * b + c, 32, stride=32), :] = result[
                32 * c : 32 * c + 32, 128 * b : 128 * b + 128
            ]
    sends = []
    for i in range(2):
        half = pl.ds(512 * i, 512)
        ready[half, :] = stage[half, :].astype(jnp.bfloat16)
        sends.append(pltpu.make_async_copy(ready.at[half], results.at[half], send_sems.at[i]))
        sends[i].start()
    loads[10].wait()
    partial[...] = jnp.dot(shared_act, w_shared_down[...], preferred_element_type=jnp.float32)

    def share(source, shift):
        at = pl.multiple_of(((tp + shift) % 4) * 512, 512)
        return source[:, pl.ds(at, 512)]

    for k, part in enumerate((part_1, part_2, part_3)):
        parts[k] = share(partial, k + 1).astype(jnp.bfloat16)
        sends.append(pltpu.make_async_copy(parts.at[k], part, send_sems.at[2 + k]))
        sends[2 + k].start()
    base[...] = share(partial, 0) + share(resid, 0).astype(jnp.float32)
    sends.append(pltpu.make_async_copy(base, base_out, send_sems.at[5]))
    sends[5].start()
    for send in sends:
        send.wait()


def run_experts(rows, own_heads, got_heads, tokens, ffn_gain, w_gate, weights):
    w_out, w_up, w_down, w_shared_gate, w_shared_up, w_shared_down = weights
    seqs, width = tokens.shape
    vmem = pl.BlockSpec(memory_space=pltpu.VMEM)
    bf16, f32 = jnp.bfloat16, jnp.float32
    part = pltpu.HBM((seqs, 512), bf16)
    hbm = pl.BlockSpec(memory_space=pltpu.HBM)
    either = pl.BlockSpec(memory_space=pl.ANY)
    return pl.pallas_call(
        expert_kernel,
        out_shape=(
            pltpu.HBM((1024, 128), bf16),
            pltpu.HBM((seqs, 512), f32),
            part,
            part,
            part,
        ),
        in_specs=[vmem] * 2 + [either] * 4 + [hbm] * 8,
        out_specs=(hbm,) * 5,
        scratch_shapes=[
            pltpu.VMEM((4, seqs, 256), bf16),
            pltpu.VMEM((seqs, 512), f32),
            pltpu.VMEM((3, seqs, 512), bf16),
            pltpu.VMEM((seqs, width), f32),
            pltpu.VMEM((seqs, width), bf16),
            pltpu.VMEM((1536, 128), f32),
            pltpu.VMEM((1024, 128), f32),
            pltpu.VMEM((1024, 128), bf16),
            pltpu.VMEM((seqs, width), bf16),
            pltpu.VMEM((1, width), f32),
            pltpu.VMEM(w_out.shape, bf16),
            pltpu.VMEM(w_up.shape[1:], bf16),
            pltpu.VMEM(w_down.shape[1:], bf16),
            pltpu.VMEM(w_shared_gate.shape, bf16),
            pltpu.VMEM(w_shared_up.shape, bf16),
            pltpu.VMEM(w_shared_down.shape, bf16),
            pltpu.SemaphoreType.DMA((11,)),
            pltpu.SemaphoreType.DMA((4,)),
            pltpu.SemaphoreType.DMA((6,)),
        ],
        compiler_params=pltpu.CompilerParams(vmem_limit_bytes=24 * 1024 * 1024),
        name="run_experts",
    )(
        rows,
        w_gate,
        *in_hbm(own_heads),
        *got_heads,
        *in_hbm(tokens, ffn_gain.reshape(1, -1), *weights),
    )


def finish_kernel(returned, combine, base, part_1, part_2, part_3, mixed, wide):
    seqs = base.shape[0]
    wide[...] = returned[...].astype(jnp.float32)
    arrived = jnp.concatenate(
        [
            jnp.concatenate(
                [
                    wide[pl.ds(2 * b + c, 128, stride=8), :].astype(jnp.bfloat16)
                    for b in range(4)
                ],
                axis=1,
            )
            for c in range(2)
        ],
        axis=0,
    )
    routed = jnp.dot(combine[...], arrived, preferred_element_type=jnp.float32)
    total = base[...]
    for part in (part_1, part_2, part_3):
        total = total + part[...].astype(jnp.float32)
    for k in range(3):
        total = total + routed[k * seqs : (k + 1) * seqs, :]
    mixed[...] = total.astype(jnp.bfloat16)


def finish(returned, combine, base, parts):
    vmem = pl.BlockSpec(memory_space=pltpu.VMEM)
    return pl.pallas_call(
        finish_kernel,
        out_shape=jax.ShapeDtypeStruct(base.shape, jnp.bfloat16),
        in_specs=[vmem] * 6,
        out_specs=vmem,
        scratch_shapes=[pltpu.VMEM((1024, 128), jnp.float32)],
        compiler_params=pltpu.CompilerParams(vmem_limit_bytes=4 * 1024 * 1024),
        name="finish",
    )(returned, combine, base, *parts)


def around(value, shift):
    count = lax.axis_size("tp")
    return lax.ppermute(value, "tp", [(i, (i + shift) % count) for i in range(count)])


def shards(
    tokens,
    kv_cache,
    lengths,
    attn_gain,
    w_query,
    w_key,
    w_value,
    lambdas,
    head_gain,
    w_out,
    ffn_gain,
    w_shared_gate,
    w_shared_up,
    w_shared_down,
    routing,
    route_weights,
    w_exp_gate,
    w_exp_up,
    w_exp_down,
):
    everyone = ("ep", "tp")
    message, heads, combine = attend(
        tokens,
        kv_cache,
        lengths,
        attn_gain,
        w_query,
        w_key,
        w_value,
        lambdas,
        head_gain,
        routing,
        route_weights,
    )
    message = message.reshape(128, 6, 2, 128)
    arrived = lax.all_to_all(message, everyone, split_axis=0, concat_axis=0, tiled=True)
    got_heads = [around(heads, k) for k in range(1, 4)]
    (gate,) = fetch(heads, (w_exp_gate,))
    rows = arrived.reshape(1536, 128)
    results, base, *parts = run_experts(
        rows,
        heads,
        got_heads,
        tokens,
        ffn_gain,
        gate,
        (w_out, w_exp_up, w_exp_down, w_shared_gate, w_shared_up, w_shared_down),
    )
    results = results.reshape(128, 4, 2, 128)
    returned = lax.all_to_all(results, everyone, split_axis=0, concat_axis=0, tiled=True)
    parts = [around(part, k + 1) for k, part in enumerate(parts)]
    combine, base = fetch(base, (combine, base))
    returned = returned.reshape(1024, 128)
    return finish(returned, combine, base, parts)


def solution(mesh):
    return jax.shard_map(
        shards,
        mesh=mesh,
        in_specs=(
            P("ep", None),
            P("ep", None, "tp"),
            P("ep"),
            P(),
            P(None, "tp"),
            P(None, "tp"),
            P(None, "tp"),
            P("tp"),
            P(),
            P(),
            P(),
            P(None, "tp"),
            P(None, "tp"),
            P("tp", None),
            P(),
            P("ep", None),
            P(("ep", "tp"), None, None),
            P(("ep", "tp"), None, None),
            P(("ep", "tp"), None, None),
        ),
        out_specs=P("ep", "tp"),
        check_vma=False,
    )
```
